128 devices in a mesh: ep: 32 (over z, y, core), tp: 4 (over x).
Axes of the slice: x: 4, y: 4, z: 4, core: 2. Of those that a mesh axis runs over, the one named last changes fastest.
Arguments:
- tokens: bfloat16 [16384, 2048], P(('ep', 'tp')), may hold values from -6 to 6
- norm_gain: float32 [2048], replicated, may hold values from 0.1 to 1.9
- expert_ids: int32 [16384, 2], P('ep'), may hold values from 0 to 31, all different within a row; in each aligned block of 128 rows (0 to 127, 128 to 255, ...) at most 10 rows name the same one
- route_weight: float32 [16384, 2], P('ep'), may hold values from 0.1 to 1
- exp_gate: bfloat16 [32, 2048, 7168], P('ep', None, 'tp'), may hold values from -0.125 to 0.125
- exp_up: bfloat16 [32, 2048, 7168], P('ep', None, 'tp'), may hold values from -0.125 to 0.125
- exp_down: bfloat16 [32, 7168, 2048], P('ep', 'tp'), may hold values from -0.0625 to 0.0625
Outputs:
- mixed: bfloat16 [16384, 2048], P(('ep', 'tp'))
The draws below stay inside these ranges and needn't reach their ends.
Inputs may be any that keep to these rules, and one draw needn't show every extreme that they name: `expert_ids`: A row names 2 different experts. Within each aligned block of 128 rows (the tokens of one device) no expert is named by more than 10 rows, and in some block one expert is named by exactly 10 rows.
All inputs are finite; a program needn't handle non-finite values.
Results may differ from the reference program's by a relative error of at most 0.012.
Values may be sent and summed in bfloat16 or wider, within the bound.
No kernel may reach another device: no remote copies, remote signals or barrier semaphores. Data moves between devices by JAX's collectives and lax.ppermute only.
A program may use at most 128 MiB of HBM per device.

```python
import math
import jax
import jax.numpy as jnp
import numpy as np
from jax import lax

D = 2048
FF = 7168
TOPK = 2
TOK_DEV = 128
EXPERTS = 32
CAP = 10
TOKENS = 16384
N_EP = 32
N_TP = 4


def level_of(stream_key, extent, cuts, smallest, largest):
    level, own = 1.0, jax.random.fold_in(stream_key, 6)
    for axis_at, shards_of in cuts:
        draws = jnp.exp(jax.random.uniform(jax.random.fold_in(own, axis_at), (shards_of,), jnp.float32, smallest / len(cuts), largest / len(cuts)))
        level = level * jnp.repeat(draws, extent[axis_at] // shards_of).reshape([-1 if axis == axis_at else 1 for axis in range(len(extent))])
    return level


def shared_out(key, own, number, rows, number_of, top, limit, slope):
    order = jax.random.permutation(key, number_of)
    crowded, ordinary = portions_of(number_of, rows * top, limit, slope, True), portions_of(number_of, rows * top, limit, slope, False)
    places = jnp.arange(number_of)

    def named(tallies, turn):
        used = int((tallies > 0).sum())
        fixed = max(1, used // 4)
        passed = fixed + (places - fixed + turn * (used - fixed)) % max(1, number_of - fixed)
        return jnp.zeros((number_of,), jnp.int32).at[order[jnp.where(places < fixed, places, passed)]].set(jnp.asarray(tallies, jnp.int32))

    tallies = jnp.where(number % 4 == 0, named(crowded, number // 4), named(ordinary, number - number // 4 - 1))
    mixed = jax.random.permutation(jax.random.fold_in(own, 3), number_of)
    donor, sink = mixed[0:number_of // 2 * 2:2], mixed[1:number_of // 2 * 2:2]
    margin = jnp.minimum(tallies[donor] - 1, limit - tallies[sink]) // 2
    margin = jnp.where((donor == order[0]) | (sink == order[0]) | (tallies[sink] == 0), 0, jnp.maximum(margin, 0))
    passed = jax.random.randint(jax.random.fold_in(own, 4), (number_of // 2,), 0, 1 << 20) % (margin + 1)
    tallies = tallies.at[donor].add(-passed).at[sink].add(passed)
    labels = jnp.searchsorted(jnp.cumsum(tallies), jnp.arange(rows * top), side="right").astype(jnp.int32)
    table = labels.reshape(top, rows).T
    table = table[jax.random.permutation(jax.random.fold_in(own, 1), rows)]
    turn = jax.random.randint(jax.random.fold_in(own, 2), (rows, 1), 0, top)
    return jnp.take_along_axis(table, (jnp.arange(top)[None, :] + turn) % top, axis=1)


def portions_of(amount, total, most, skew, full):
    loads = [(1 << 20) // math.isqrt(standing ** skew) + 1 for standing in range(1, amount + 1)]
    largest = most if full else min(most, max(-(-total // amount), total * loads[0] // sum(loads)))
    least = 1 if total - largest >= amount - 1 else 0
    holding, spare = [largest] + [least] * (amount - 1), total - largest - least * (amount - 1)
    while spare > 0:
        candidates = [i for i in range(1, amount) if holding[i] < largest] or [i for i in range(1, amount) if holding[i] < most]
        mass, remaining = sum([loads[i] for i in candidates]), spare
        for i in candidates:
            more = min(most - holding[i], max(1, remaining * loads[i] // mass), spare)
            holding[i] = holding[i] + more
            spare = spare - more
    return np.array(holding)


def gaussian(own_key, shape, spread, limit, cuts=(), kind=jnp.bfloat16):
    array = jax.random.normal(own_key, shape, jnp.float32) * spread
    if len(cuts) > 0:
        array = level_of(own_key, shape, cuts, -0.22, 0.18) * array
    return jnp.clip(array, min=-limit, max=limit).astype(kind)


def setup_inputs(seed: int = 0) -> dict:
    keys = jax.random.split(jax.random.key(seed), 8)
    tokens = gaussian(keys[0], (TOKENS, D), 1.0, 6.0, ((0, 128),))
    norm_gain = jnp.clip(1.0 + 0.18 * jax.random.normal(keys[1], (D,), jnp.float32), 0.1, 1.9)
    expert_ids_keys = jax.random.split(jax.random.fold_in(keys[2], 1), TOKENS // TOK_DEV)
    expert_ids_turns = jax.random.permutation(jax.random.fold_in(keys[2], 3), TOKENS // TOK_DEV)
    expert_ids = jax.vmap(lambda own, number: shared_out(jax.random.fold_in(keys[2], 2), own, number, TOK_DEV, EXPERTS, TOPK, CAP, 2))(expert_ids_keys, expert_ids_turns).reshape((TOKENS, TOPK))
    route_weight = jnp.clip(0.1 + 0.9 * jax.random.uniform(keys[3], (TOKENS, TOPK), jnp.float32) ** level_of(keys[3], (TOKENS, TOPK), ((0, 32),), -0.2, 0.2), 0.1, 1.0)
    exp_gate = gaussian(keys[4], (EXPERTS, D, FF), D ** -0.5, 0.125, ((0, 32), (2, 4)))
    exp_up = gaussian(keys[5], (EXPERTS, D, FF), D ** -0.5, 0.125, ((0, 32), (2, 4)))
    exp_down = gaussian(keys[6], (EXPERTS, FF, D), FF ** -0.5, 0.0625, ((0, 32), (1, 4)))
    return {"tokens": tokens, "norm_gain": norm_gain, "expert_ids": expert_ids, "route_weight": route_weight, "exp_gate": exp_gate, "exp_up": exp_up, "exp_down": exp_down}


norm_eps = 1e-05

def normalize(tokens, norm_gain):
    values = tokens.astype(jnp.float32)
    factor = lax.rsqrt(lax.optimization_barrier(jnp.mean(values * values, axis=-1, keepdims=True)) + norm_eps)
    return (values * factor * norm_gain.astype(jnp.float32)).astype(jnp.bfloat16)

def count_slots(flat_ids, experts_all):
    onehot = (flat_ids[..., None] == jnp.arange(experts_all, dtype=jnp.int32)).astype(jnp.int32)
    before = jnp.cumsum(onehot, axis=1) - onehot
    return lax.optimization_barrier(jnp.sum(before * onehot, axis=-1)).astype(jnp.int32)

def reference(tokens, norm_gain, expert_ids, route_weight, exp_gate, exp_up, exp_down):
    devices_all = N_EP * N_TP
    normed = normalize(tokens, norm_gain)
    slots = count_slots(expert_ids.reshape(devices_all, TOK_DEV * TOPK), EXPERTS).reshape(TOKENS, TOPK)
    device_of = (jnp.arange(TOKENS, dtype=jnp.int32) // TOK_DEV)[:, None]
    where_buf = (device_of * CAP + slots).astype(jnp.int32)
    spare = devices_all * CAP
    block_ff = FF // N_TP

    def one_expert(mixed, inputs):
        index, w_gate, w_up, w_down = inputs
        chosen = expert_ids == index
        target = jnp.where(chosen, where_buf, spare).astype(jnp.int32)
        filled = jnp.zeros((spare + 1, D), jnp.bfloat16)
        for column in range(TOPK):
            filled = filled.at[target[:, column]].set(normed)
        filled = filled[:spare]
        gate = jnp.dot(filled, w_gate, preferred_element_type=jnp.float32)
        up_val = jnp.dot(filled, w_up, preferred_element_type=jnp.float32)
        hidden = (jax.nn.silu(gate) * up_val).astype(jnp.bfloat16)
        summed = jnp.zeros((spare, D), jnp.float32)
        for blockno in range(N_TP):
            part = jnp.dot(hidden[:, blockno * block_ff:(blockno + 1) * block_ff], w_down[blockno * block_ff:(blockno + 1) * block_ff], preferred_element_type=jnp.float32).astype(jnp.bfloat16)
            summed = summed + part.astype(jnp.float32)
        expert_out = summed.astype(jnp.bfloat16)
        safe = jnp.where(chosen, where_buf, 0).astype(jnp.int32)
        for column in range(TOPK):
            picked = expert_out[safe[:, column]].astype(jnp.float32)
            weight = jnp.where(chosen[:, column], route_weight[:, column], jnp.float32(0.0))
            mixed = mixed + weight[:, None] * picked
        return (mixed, None)
    start = jnp.zeros((TOKENS, D), jnp.float32)
    mixed, unused = lax.scan(one_expert, start, (jnp.arange(EXPERTS, dtype=jnp.int32), exp_gate, exp_up, exp_down))
    return mixed.astype(jnp.bfloat16)
```

```python
import jax
import jax.numpy as jnp
from jax import lax
from jax.sharding import Mesh
from jax.sharding import PartitionSpec as P

TOPK = 2
TOK_DEV = 128
EP = ("ep_0", "ep_1", "ep_2")
EP_TP = ("ep_0", "ep_1", "ep_2", "tp")
CHUNKS = (5, 5)
LANES = 128


norm_eps = 1e-05


def normalize(tokens, norm_gain):
    values = tokens.astype(jnp.float32)
    factor = lax.rsqrt(jnp.mean(values * values, axis=-1, keepdims=True) + norm_eps)
    return (values * factor * norm_gain).astype(jnp.bfloat16)


def shift(value, by):
    size = lax.axis_size("tp")
    return lax.ppermute(value, "tp", [(i, (i + by) % size) for i in range(size)])


def exchange(rows, per_peer):
    ep_size = lax.axis_size(EP)
    width = rows.shape[-1]
    fine = rows.reshape(ep_size, per_peer * (width // LANES), LANES)
    return lax.all_to_all(fine, EP, 0, 0, tiled=True).reshape(rows.shape)


def gather_tp(rows):
    half = rows.shape[0] // 2
    from_left = shift(rows, 1)
    from_right = shift(rows, -1)
    far_a = shift(from_left[:half], 1)
    far_b = shift(from_right[half:], -1)
    return jnp.concatenate([rows, from_left, from_right, far_a, far_b], axis=0)


def add_rounded(a, b):
    return (a.astype(jnp.float32) + b.astype(jnp.float32)).astype(jnp.bfloat16)


def scatter_tp(parts):
    rows = parts.shape[0] // 4
    half = rows // 2
    own, to_left, to_right, far = (parts[i * rows : (i + 1) * rows] for i in range(4))
    via_right = shift(far[:half], -1)
    via_left = shift(far[half:], 1)
    left = jnp.concatenate([add_rounded(to_left[:half], via_right), to_left[half:]], axis=0)
    right = jnp.concatenate([to_right[:half], add_rounded(to_right[half:], via_left)], axis=0)
    got_a = shift(left, -1)
    got_b = shift(right, 1)
    total = own.astype(jnp.float32) + got_a.astype(jnp.float32) + got_b.astype(jnp.float32)
    return total.astype(jnp.bfloat16)


def expert(rows, w_gate, w_up, w_down):
    gate = jnp.dot(rows, w_gate, preferred_element_type=jnp.float32)
    up_val = jnp.dot(rows, w_up, preferred_element_type=jnp.float32)
    hidden = (jax.nn.silu(gate) * up_val).astype(jnp.bfloat16)
    return jnp.dot(hidden, w_down, preferred_element_type=jnp.float32).astype(jnp.bfloat16)


def per_device(tokens, norm_gain, expert_ids, route_weight, exp_gate, exp_up, exp_down):
    experts_all = lax.axis_size(EP)
    tok_count = tokens.shape[0]
    offset = lax.axis_index("tp") * tok_count
    ids = lax.dynamic_slice_in_dim(expert_ids, offset, tok_count, 0)
    weight = lax.dynamic_slice_in_dim(route_weight, offset, tok_count, 0)
    normed = normalize(tokens, norm_gain)

    hits = ids[:, :, None] == jnp.arange(experts_all, dtype=jnp.int32)
    named = jnp.any(hits, axis=1)
    at = jnp.arange(tok_count, dtype=jnp.int32)
    earlier = (at[:, None] > at[None, :]).astype(jnp.bfloat16)
    slot = jnp.dot(earlier, named.astype(jnp.bfloat16), preferred_element_type=jnp.float32)
    slot = jnp.where(named, slot.astype(jnp.int32), -1)
    mass = jnp.sum(jnp.where(hits, weight[:, :, None], 0.0), axis=1)

    firsts = [sum(CHUNKS[:i]) for i in range(len(CHUNKS))]
    outs = []
    arrived = []
    picks = []
    for first, count in zip(firsts, CHUNKS):
        which = first + jnp.arange(count, dtype=jnp.int32)
        pick = slot[:, :, None] == which
        picks.append(pick)
        chosen = pick.astype(jnp.bfloat16).reshape(tok_count, experts_all * count)
        sent = lax.dot_general(
            chosen, normed, (((0,), (0,)), ((), ())), preferred_element_type=jnp.float32
        ).astype(jnp.bfloat16)
        arrived.append(exchange(sent, count))
    total = jnp.zeros(tokens.shape, jnp.float32)
    for pick, count, rows in zip(picks, CHUNKS, arrived):
        parts = expert(gather_tp(rows), exp_gate[0], exp_up[0], exp_down[0])
        returned = exchange(scatter_tp(parts), count)
        spread = jnp.where(pick, mass[:, :, None], 0.0).reshape(tok_count, experts_all * count)
        high = spread.astype(jnp.bfloat16)
        low = (spread - high.astype(jnp.float32)).astype(jnp.bfloat16)
        total = total + jnp.dot(high, returned, preferred_element_type=jnp.float32)
        total = total + jnp.dot(low, returned, preferred_element_type=jnp.float32)
    return total.astype(jnp.bfloat16)


def solution(mesh):
    finer = Mesh(mesh.devices.reshape(4, 4, 2, mesh.shape["tp"]), ("ep_0", "ep_1", "ep_2", "tp"))
    return jax.shard_map(
        per_device,
        mesh=finer,
        in_specs=(
            P(EP_TP, None),
            P(),
            P(EP, None),
            P(EP, None),
            P(EP, None, "tp"),
            P(EP, None, "tp"),
            P(EP, "tp", None),
        ),
        out_specs=P(EP_TP, None),
        check_vma=False,
    )
```

```python
import functools

import jax
import jax.numpy as jnp
from jax import lax
from jax.experimental import pallas as pl
from jax.experimental.pallas import tpu as pltpu
from jax.sharding import Mesh
from jax.sharding import PartitionSpec as P

EP = ("ep_0", "ep_1", "ep_2")
EP_TP = ("ep_0", "ep_1", "ep_2", "tp")
CAP = 10
EARLY = 8
LATE = CAP - EARLY
OFFSETS = (0, -1, 1, 2)
UP_TILE = 256
DOWN_TILE = 1024
MIB = 2**20


norm_eps = 1e-05
VMEM_SPEC = pl.BlockSpec(memory_space=pltpu.VMEM)
HBM_SPEC = pl.BlockSpec(memory_space=pltpu.HBM)


def normalize(tokens, norm_gain):
    values = tokens.astype(jnp.float32)
    factor = lax.rsqrt(jnp.mean(values * values, axis=-1, keepdims=True) + norm_eps)
    return (values * factor * norm_gain).astype(jnp.bfloat16)


def shift(value, by):
    size = lax.axis_size("tp")
    return lax.ppermute(value, "tp", [(i, (i + by) % size) for i in range(size)])


def exchange(rows):
    ep_size = lax.axis_size(EP)
    tiles = rows.reshape(ep_size, rows.shape[0] // ep_size, rows.shape[1])
    return lax.all_to_all(tiles, EP, 0, 0, tiled=True).reshape(rows.shape)


def gather_tp(rows):
    half = rows.shape[0] // 2
    from_left = shift(rows, 1)
    from_right = shift(rows, -1)
    far_a = shift(from_left[:half], 1)
    far_b = shift(from_right[half:], -1)
    return rows, from_left, from_right, far_a, far_b


def add_rounded(a, b):
    return (a.astype(jnp.float32) + b.astype(jnp.float32)).astype(jnp.bfloat16)


def place(target, blocks):
    at = 0
    for b in blocks:
        target[at : at + b.shape[0], :] = b[...]
        at += b.shape[0]


def cut(value, outs, columns=slice(None)):
    at = 0
    for o in outs:
        o[:, columns] = value[at : at + o.shape[0]].astype(o.dtype)
        at += o.shape[0]


def expert_kernel(n_in, n_out, *refs):
    blocks = refs[:n_in]
    w_gate, w_up, w_down = refs[n_in : n_in + 3]
    outs = refs[n_in + 3 : n_in + 3 + n_out]
    rows, hidden, gates, ups, gate_tiles, up_tiles, down_tiles, sems = refs[n_in + 3 + n_out :]
    steps, downs = gate_tiles.shape[0], down_tiles.shape[0]

    def cols(t, width):
        return pl.ds(pl.multiple_of(t * width, width), width)

    def load(kind, t):
        src, dst = ((w_gate, gate_tiles), (w_up, up_tiles), (w_down, down_tiles))[kind]
        return pltpu.make_async_copy(
            src.at[0, :, cols(t, dst.shape[2])], dst.at[t], sems.at[kind, t]
        )

    def start_up(t, c):
        load(0, t).start()
        load(1, t).start()
        return c

    def start_down(t, c):
        load(2, t).start()
        return c

    lax.fori_loop(0, steps, start_up, 0)
    lax.fori_loop(0, downs, start_down, 0)
    place(rows, blocks)

    def multiply(t):
        load(0, t).wait()
        load(1, t).wait()
        gate = jnp.dot(rows[...], gate_tiles[t], preferred_element_type=jnp.float32)
        up = jnp.dot(rows[...], up_tiles[t], preferred_element_type=jnp.float32)
        return gate, up

    def activate(t):
        gate, up = gates[t % 2], ups[t % 2]
        value = (gate / (1.0 + jnp.exp(-gate)) * up).astype(jnp.bfloat16)
        hidden[:, cols(t, UP_TILE)] = value

    def up_step(t, c):
        gate, up = multiply(t)
        activate(t - 1)
        gates[t % 2] = gate
        ups[t % 2] = up
        return c

    gates[0], ups[0] = multiply(0)
    lax.fori_loop(1, steps, up_step, 0)
    activate(steps - 1)

    def down_step(t, c):
        load(2, t).wait()
        part = jnp.dot(hidden[...], down_tiles[t], preferred_element_type=jnp.float32)
        cut(part, outs, cols(t, DOWN_TILE))
        return c

    lax.fori_loop(0, downs, down_step, 0)


def expert(blocks, sizes, w_gate, w_up, w_down):
    d, ff = w_gate.shape[1:]
    m = sum(b.shape[0] for b in blocks)
    steps, downs = ff // UP_TILE, d // DOWN_TILE
    return pl.pallas_call(
        functools.partial(expert_kernel, len(blocks), len(sizes)),
        in_specs=[VMEM_SPEC] * len(blocks) + [HBM_SPEC] * 3,
        out_specs=[VMEM_SPEC] * len(sizes),
        out_shape=[jax.ShapeDtypeStruct((s, d), jnp.bfloat16) for s in sizes],
        scratch_shapes=[
            pltpu.VMEM((m, d), jnp.bfloat16),
            pltpu.VMEM((m, ff), jnp.bfloat16),
            pltpu.VMEM((2, m, UP_TILE), jnp.float32),
            pltpu.VMEM((2, m, UP_TILE), jnp.float32),
            pltpu.VMEM((steps, d, UP_TILE), jnp.bfloat16),
            pltpu.VMEM((steps, d, UP_TILE), jnp.bfloat16),
            pltpu.VMEM((downs, ff, DOWN_TILE), jnp.bfloat16),
            pltpu.SemaphoreType.DMA((3, max(steps, downs))),
        ],
        compiler_params=pltpu.CompilerParams(vmem_limit_bytes=58 * MIB),
        cost_estimate=pl.CostEstimate(
            flops=6 * m * d * ff, bytes_accessed=6 * d * ff + 4 * m * d, transcendentals=m * ff
        ),
    )(*blocks, w_gate, w_up, w_down)


def select_kernel(chosen, *refs):
    blocks, out, rows = refs[:-2], refs[-2], refs[-1]
    place(rows, blocks)
    out[...] = jnp.dot(chosen[...], rows[...], preferred_element_type=jnp.float32).astype(out.dtype)


def select_rows(chosen, blocks):
    d = blocks[0].shape[1]
    n, m = chosen.shape
    return pl.pallas_call(
        select_kernel,
        in_specs=[VMEM_SPEC] * (1 + len(blocks)),
        out_specs=VMEM_SPEC,
        out_shape=jax.ShapeDtypeStruct((n, d), jnp.bfloat16),
        scratch_shapes=[pltpu.VMEM((m, d), jnp.bfloat16)],
        compiler_params=pltpu.CompilerParams(vmem_limit_bytes=16 * MIB),
        cost_estimate=pl.CostEstimate(
            flops=2 * n * m * d, bytes_accessed=2 * d * (n + m), transcendentals=0
        ),
    )(chosen, *blocks)


def weigh_kernel(high, low, rows, *outs):
    value = jnp.dot(high[...], rows[...], preferred_element_type=jnp.float32)
    value = value + jnp.dot(low[...], rows[...], preferred_element_type=jnp.float32)
    cut(value, outs)


def weigh_rows(weights, rows, sizes):
    n, m = weights.shape
    d = rows.shape[1]
    high = weights.astype(jnp.bfloat16)
    low = (weights - high.astype(jnp.float32)).astype(jnp.bfloat16)
    return pl.pallas_call(
        weigh_kernel,
        in_specs=[VMEM_SPEC] * 3,
        out_specs=[VMEM_SPEC] * len(sizes),
        out_shape=[jax.ShapeDtypeStruct((s, d), jnp.bfloat16) for s in sizes],
        compiler_params=pltpu.CompilerParams(vmem_limit_bytes=24 * MIB),
        cost_estimate=pl.CostEstimate(
            flops=4 * n * m * d, bytes_accessed=2 * d * (n + m), transcendentals=0
        ),
    )(high, low, rows)


def finish_kernel(high, low, rows, own, near_a, near_b, far_a, far_b, out):
    value = jnp.dot(high[...], rows[...], preferred_element_type=jnp.float32)
    value = value + jnp.dot(low[...], rows[...], preferred_element_type=jnp.float32)
    value = value + own[...].astype(jnp.float32)
    half = out.shape[0] // 2
    top = near_a[...].astype(jnp.float32) + far_a[...].astype(jnp.float32)
    bottom = near_b[...].astype(jnp.float32) + far_b[...].astype(jnp.float32)
    out[:half, :] = (value[:half] + top).astype(out.dtype)
    out[half:, :] = (value[half:] + bottom).astype(out.dtype)


def finish(weights, rows, own, pieces):
    n, m = weights.shape
    d = rows.shape[1]
    high = weights.astype(jnp.bfloat16)
    low = (weights - high.astype(jnp.float32)).astype(jnp.bfloat16)
    return pl.pallas_call(
        finish_kernel,
        in_specs=[VMEM_SPEC] * 8,
        out_specs=VMEM_SPEC,
        out_shape=jax.ShapeDtypeStruct((n, d), jnp.bfloat16),
        compiler_params=pltpu.CompilerParams(vmem_limit_bytes=16 * MIB),
        cost_estimate=pl.CostEstimate(
            flops=4 * n * m * d, bytes_accessed=2 * d * (n + m), transcendentals=0
        ),
    )(high, low, rows, own, *pieces)


def send_near(to_left, to_right):
    got_bottom = shift(to_left[1], -1)
    got_top = shift(to_right[0], 1)
    return got_top, got_bottom


def send_far(to_left, to_right, far):
    via_right = shift(far[0], -1)
    via_left = shift(far[1], 1)
    got_top = shift(add_rounded(to_left[0], via_right), -1)
    got_bottom = shift(add_rounded(to_right[1], via_left), 1)
    return got_top, got_bottom


def per_device(tokens, norm_gain, expert_ids, route_weight, exp_gate, exp_up, exp_down):
    experts_all = lax.axis_size(EP)
    tok_count, width = tokens.shape
    half = tok_count // 2
    me = lax.axis_index("tp")
    size = lax.axis_size("tp")

    def block_of(value, by):
        return lax.dynamic_slice_in_dim(value, ((me + by + size) % size) * tok_count, tok_count, 0)

    def slots_of(ids):
        hits = ids.T[:, None, :] == jnp.arange(experts_all, dtype=jnp.int32)[:, None]
        named = jnp.any(hits, axis=0)
        at = jnp.arange(tok_count, dtype=jnp.int32)
        earlier = (at[:, None] < at[None, :]).astype(jnp.bfloat16)
        rank = jnp.dot(named.astype(jnp.bfloat16), earlier, preferred_element_type=jnp.float32)
        return jnp.where(named, rank.astype(jnp.int32), -1), hits

    own_ids = block_of(expert_ids, 0)
    own_slot, own_hits = slots_of(own_ids)
    normed = normalize(tokens, norm_gain)
    early = own_slot[:, None, :] == jnp.arange(EARLY, dtype=jnp.int32)[:, None]
    chosen = early.astype(jnp.bfloat16).reshape(experts_all * EARLY, tok_count)
    arrived = exchange(
        jnp.dot(chosen, normed, preferred_element_type=jnp.float32).astype(jnp.bfloat16)
    )
    arrived, *blocks = lax.optimization_barrier((arrived, *gather_tp(normed)))

    masks, masses = [], []
    for at, by in enumerate(OFFSETS):
        ids, weight = block_of(expert_ids, by), block_of(route_weight, by)
        slot, hits = slots_of(ids)
        masses.append(jnp.sum(jnp.where(hits, weight.T[:, None, :], 0.0), axis=0))
        wanted = jnp.full((len(OFFSETS), LATE), -2, jnp.int32)
        wanted = wanted.at[at].set(EARLY + jnp.arange(LATE, dtype=jnp.int32)).reshape(-1)
        masks.append(slot[:, None, :] == wanted[:, None])
    late = jnp.concatenate(masks, axis=2)
    late_rows = experts_all * len(OFFSETS) * LATE
    late_mass = jnp.where(late, jnp.concatenate(masses, axis=1)[:, None, :], 0.0)
    late_mass = late_mass.reshape(late_rows, len(OFFSETS) * tok_count)
    early_mass = jnp.where(early, masses[0][:, None, :], 0.0).reshape(experts_all * EARLY, tok_count)
    late_chosen = late.astype(jnp.bfloat16).reshape(late_rows, len(OFFSETS) * tok_count)
    late_arrived = exchange(select_rows(late_chosen, blocks))

    weights = (exp_gate, exp_up, exp_down)
    count = arrived.shape[0]
    mid = count // 2
    own_rows, left_rows, right_rows, far_a, far_b = gather_tp(arrived)
    (own_part,) = expert([own_rows], [count], *weights)
    left_rows, right_rows, own_part = lax.optimization_barrier((left_rows, right_rows, own_part))
    parts = expert([left_rows, right_rows], [mid] * 4, *weights)
    to_left, to_right = parts[:2], parts[2:]
    near = send_near(to_left, to_right)
    far_a, far_b, to_left, to_right = lax.optimization_barrier((far_a, far_b, to_left, to_right))
    far_parts = expert([far_a, far_b], [mid] * 2, *weights)
    late_arrived, far_parts = lax.optimization_barrier((late_arrived, far_parts))
    far = send_far(to_left, to_right, far_parts)
    (late_part,) = expert([late_arrived], [late_rows], *weights)
    late_back = exchange(late_part)

    sums = weigh_rows(late_mass.T, late_back, [tok_count] + [half] * 6)
    token_near = send_near(sums[1:3], sums[3:5])
    token_far = send_far(sums[1:3], sums[3:5], sums[5:7])

    summed = jnp.concatenate([near[0], near[1]], axis=0).astype(jnp.float32)
    summed = summed + jnp.concatenate([far[0], far[1]], axis=0).astype(jnp.float32)
    summed = (summed + own_part.astype(jnp.float32)).astype(jnp.bfloat16)
    back = exchange(summed)
    return finish(early_mass.T, back, sums[0], token_near + token_far)


def solution(mesh):
    finer = Mesh(mesh.devices.reshape(4, 4, 2, mesh.shape["tp"]), ("ep_0", "ep_1", "ep_2", "tp"))
    return jax.shard_map(
        per_device,
        mesh=finer,
        in_specs=(
            P(EP_TP, None),
            P(),
            P(EP, None),
            P(EP, None),
            P(EP, None, "tp"),
            P(EP, None, "tp"),
            P(EP, "tp", None),
        ),
        out_specs=P(EP_TP, None),
        check_vma=False,
    )
```

```python
import functools

import jax
import jax.numpy as jnp
from jax import lax
from jax.experimental import pallas as pl
from jax.experimental.pallas import tpu as pltpu
from jax.sharding import Mesh
from jax.sharding import PartitionSpec as P


EP = ("ep_0", "ep_1", "ep_2")
EP_TP = ("ep_0", "ep_1", "ep_2", "tp")
CAP = 10
EARLY = 8
LATE = CAP - EARLY
OFFSETS = (0, -1, 1, 2)
UP_TILE = 256
DOWN_TILE = 1024
MIB = 2**20


norm_eps = 1e-05
VMEM_SPEC = pl.BlockSpec(memory_space=pltpu.VMEM)
HBM_SPEC = pl.BlockSpec(memory_space=pltpu.HBM)


def normalize(tokens, norm_gain):
    values = tokens.astype(jnp.float32)
    factor = lax.rsqrt(jnp.mean(values * values, axis=-1, keepdims=True) + norm_eps)
    return (values * factor * norm_gain).astype(jnp.bfloat16)


def shift(value, by):
    size = lax.axis_size("tp")
    return lax.ppermute(value, "tp", [(i, (i + by) % size) for i in range(size)])


def exchange(rows):
    ep_size = lax.axis_size(EP)
    tiles = rows.reshape(ep_size, rows.shape[0] // ep_size, rows.shape[1])
    return lax.all_to_all(tiles, EP, 0, 0, tiled=True).reshape(rows.shape)


def gather_tp(rows):
    half = rows.shape[0] // 2
    from_left = shift(rows, 1)
    from_right = shift(rows, -1)
    far_a = shift(from_left[:half], 1)
    far_b = shift(from_right[half:], -1)
    return rows, from_left, from_right, far_a, far_b


def add_rounded(a, b):
    return (a.astype(jnp.float32) + b.astype(jnp.float32)).astype(jnp.bfloat16)


def place(target, blocks):
    at = 0
    for b in blocks:
        target[at : at + b.shape[0], :] = b[...]
        at += b.shape[0]


def cut(value, outs, columns=slice(None)):
    at = 0
    for o in outs:
        o[:, columns] = value[at : at + o.shape[0]].astype(o.dtype)
        at += o.shape[0]


def expert_rows(rows, hidden, gates, ups, up_tiles, down_tile, outs):
    steps, downs = hidden.shape[1] // UP_TILE, outs[0].shape[1] // DOWN_TILE

    def cols(t, width):
        return pl.ds(pl.multiple_of(t * width, width), width)

    def multiply(t):
        w_gate, w_up = up_tiles(t)
        gate = jnp.dot(rows[...], w_gate[...], preferred_element_type=jnp.float32)
        up = jnp.dot(rows[...], w_up[...], preferred_element_type=jnp.float32)
        return gate, up

    def activate(t):
        gate, up = gates[t % 2], ups[t % 2]
        value = (gate / (1.0 + jnp.exp(-gate)) * up).astype(jnp.bfloat16)
        hidden[:, cols(t, UP_TILE)] = value

    def up_step(t, c):
        gate, up = multiply(t)
        activate(t - 1)
        gates[t % 2] = gate
        ups[t % 2] = up
        return c

    gates[0], ups[0] = multiply(0)
    lax.fori_loop(1, steps, up_step, 0)
    activate(steps - 1)

    def down_step(t, c):
        part = jnp.dot(hidden[...], down_tile(t)[...], preferred_element_type=jnp.float32)
        cut(part, outs, cols(t, DOWN_TILE))
        return c

    lax.fori_loop(0, downs, down_step, 0)


def stream_kernel(block, w_gate, w_up, w_down, out, gate_tiles, up_tiles, down_tiles, *scratch):
    rows, hidden, gates, ups, sems = scratch

    def load(kind, t):
        src, dst = ((w_gate, gate_tiles), (w_up, up_tiles), (w_down, down_tiles))[kind]
        width = dst.shape[2]
        at = pl.ds(pl.multiple_of(t * width, width), width)
        return pltpu.make_async_copy(src.at[0, :, at], dst.at[t], sems.at[kind, t])

    def start_up(t, c):
        load(0, t).start()
        load(1, t).start()
        return c

    def start_down(t, c):
        load(2, t).start()
        return c

    lax.fori_loop(0, gate_tiles.shape[0], start_up, 0)
    lax.fori_loop(0, down_tiles.shape[0], start_down, 0)
    place(rows, [block])

    def up_tiles_of(t):
        load(0, t).wait()
        load(1, t).wait()
        return gate_tiles.at[t], up_tiles.at[t]

    def down_tile_of(t):
        load(2, t).wait()
        return down_tiles.at[t]

    expert_rows(rows, hidden, gates, ups, up_tiles_of, down_tile_of, [out])


def kept_kernel(n_in, *refs):
    blocks = refs[:n_in]
    gate_tiles, up_tiles, down_tiles = refs[n_in : n_in + 3]
    outs = refs[n_in + 3 : -4]
    rows, hidden, gates, ups = refs[-4:]
    place(rows, blocks)
    expert_rows(
        rows,
        hidden,
        gates,
        ups,
        lambda t: (gate_tiles.at[t], up_tiles.at[t]),
        lambda t: down_tiles.at[t],
        outs,
    )


def expert_cost(m, d, ff, weights):
    return pl.CostEstimate(
        flops=6 * m * d * ff, bytes_accessed=6 * d * ff * weights + 4 * m * d, transcendentals=m * ff
    )


def row_buffers(m, d, ff):
    return [
        pltpu.VMEM((m, d), jnp.bfloat16),
        pltpu.VMEM((m, ff), jnp.bfloat16),
        pltpu.VMEM((2, m, UP_TILE), jnp.float32),
        pltpu.VMEM((2, m, UP_TILE), jnp.float32),
    ]


def expert_streamed(rows, weights, keep):
    d, ff = weights[0].shape[1:]
    m = rows.shape[0]
    steps, downs = ff // UP_TILE, d // DOWN_TILE
    tiles = [
        pltpu.VMEM((steps, d, UP_TILE), jnp.bfloat16),
        pltpu.VMEM((steps, d, UP_TILE), jnp.bfloat16),
        pltpu.VMEM((downs, ff, DOWN_TILE), jnp.bfloat16),
    ]
    return pl.pallas_call(
        stream_kernel,
        in_specs=[VMEM_SPEC] + [HBM_SPEC] * 3,
        out_specs=[VMEM_SPEC] * (4 if keep else 1),
        out_shape=[jax.ShapeDtypeStruct((m, d), jnp.bfloat16)] + (tiles if keep else []),
        scratch_shapes=([] if keep else tiles)
        + row_buffers(m, d, ff)
        + [pltpu.SemaphoreType.DMA((3, max(steps, downs)))],
        compiler_params=pltpu.CompilerParams(vmem_limit_bytes=(12 if keep else 34) * MIB),
        cost_estimate=expert_cost(m, d, ff, 1),
    )(rows, *(pltpu.with_memory_space_constraint(w, pltpu.HBM) for w in weights))


def expert_kept(blocks, sizes, tiles):
    steps, d = tiles[0].shape[:2]
    ff = steps * UP_TILE
    m = sum(b.shape[0] for b in blocks)
    return pl.pallas_call(
        functools.partial(kept_kernel, len(blocks)),
        in_specs=[VMEM_SPEC] * (len(blocks) + 3),
        out_specs=[VMEM_SPEC] * len(sizes),
        out_shape=[jax.ShapeDtypeStruct((s, d), jnp.bfloat16) for s in sizes],
        scratch_shapes=row_buffers(m, d, ff),
        compiler_params=pltpu.CompilerParams(vmem_limit_bytes=12 * MIB),
        cost_estimate=expert_cost(m, d, ff, 0),
    )(*blocks, *(pltpu.with_memory_space_constraint(w, pltpu.VMEM) for w in tiles))


def select_kernel(chosen, *refs):
    blocks, out, rows = refs[:-2], refs[-2], refs[-1]
    place(rows, blocks)
    out[...] = jnp.dot(chosen[...], rows[...], preferred_element_type=jnp.float32).astype(out.dtype)


def select_rows(chosen, blocks):
    d = blocks[0].shape[1]
    n, m = chosen.shape
    return pl.pallas_call(
        select_kernel,
        in_specs=[VMEM_SPEC] * (1 + len(blocks)),
        out_specs=VMEM_SPEC,
        out_shape=jax.ShapeDtypeStruct((n, d), jnp.bfloat16),
        scratch_shapes=[pltpu.VMEM((m, d), jnp.bfloat16)],
        compiler_params=pltpu.CompilerParams(vmem_limit_bytes=16 * MIB),
        cost_estimate=pl.CostEstimate(
            flops=2 * n * m * d, bytes_accessed=2 * d * (n + m), transcendentals=0
        ),
    )(chosen, *blocks)


def weigh_kernel(high, low, rows, *outs):
    value = jnp.dot(high[...], rows[...], preferred_element_type=jnp.float32)
    value = value + jnp.dot(low[...], rows[...], preferred_element_type=jnp.float32)
    cut(value, outs)


def weigh_rows(weights, rows, sizes):
    n, m = weights.shape
    d = rows.shape[1]
    high = weights.astype(jnp.bfloat16)
    low = (weights - high.astype(jnp.float32)).astype(jnp.bfloat16)
    return pl.pallas_call(
        weigh_kernel,
        in_specs=[VMEM_SPEC] * 3,
        out_specs=[VMEM_SPEC] * len(sizes),
        out_shape=[jax.ShapeDtypeStruct((s, d), jnp.bfloat16) for s in sizes],
        compiler_params=pltpu.CompilerParams(vmem_limit_bytes=24 * MIB),
        cost_estimate=pl.CostEstimate(
            flops=4 * n * m * d, bytes_accessed=2 * d * (n + m), transcendentals=0
        ),
    )(high, low, rows)


def finish_kernel(high, low, rows, own, near_a, near_b, far_a, far_b, out):
    value = jnp.dot(high[...], rows[...], preferred_element_type=jnp.float32)
    value = value + jnp.dot(low[...], rows[...], preferred_element_type=jnp.float32)
    value = value + own[...].astype(jnp.float32)
    half = out.shape[0] // 2
    top = near_a[...].astype(jnp.float32) + far_a[...].astype(jnp.float32)
    bottom = near_b[...].astype(jnp.float32) + far_b[...].astype(jnp.float32)
    out[:half, :] = (value[:half] + top).astype(out.dtype)
    out[half:, :] = (value[half:] + bottom).astype(out.dtype)


def finish(weights, rows, own, pieces):
    n, m = weights.shape
    d = rows.shape[1]
    high = weights.astype(jnp.bfloat16)
    low = (weights - high.astype(jnp.float32)).astype(jnp.bfloat16)
    return pl.pallas_call(
        finish_kernel,
        in_specs=[VMEM_SPEC] * 8,
        out_specs=VMEM_SPEC,
        out_shape=jax.ShapeDtypeStruct((n, d), jnp.bfloat16),
        compiler_params=pltpu.CompilerParams(vmem_limit_bytes=16 * MIB),
        cost_estimate=pl.CostEstimate(
            flops=4 * n * m * d, bytes_accessed=2 * d * (n + m), transcendentals=0
        ),
    )(high, low, rows, own, *pieces)


def send_near(to_left, to_right):
    got_bottom = shift(to_left, -1)
    got_top = shift(to_right, 1)
    return got_top, got_bottom


def send_far(far_top, far_bottom):
    return shift(far_top, -1), shift(far_bottom, 1)


def send_on(to_left, to_right, via_right, via_left):
    got_top = shift(add_rounded(to_left, via_right), -1)
    got_bottom = shift(add_rounded(to_right, via_left), 1)
    return got_top, got_bottom


def per_device(tokens, norm_gain, expert_ids, route_weight, exp_gate, exp_up, exp_down):
    experts_all = lax.axis_size(EP)
    tok_count, _ = tokens.shape
    half = tok_count // 2
    me = lax.axis_index("tp")
    size = lax.axis_size("tp")

    def block_of(value, by):
        return lax.dynamic_slice_in_dim(value, ((me + by + size) % size) * tok_count, tok_count, 0)

    def slots_of(ids):
        hits = ids.T[:, None, :] == jnp.arange(experts_all, dtype=jnp.int32)[:, None]
        named = jnp.any(hits, axis=0)
        at = jnp.arange(tok_count, dtype=jnp.int32)
        earlier = (at[:, None] < at[None, :]).astype(jnp.bfloat16)
        rank = jnp.dot(named.astype(jnp.bfloat16), earlier, preferred_element_type=jnp.float32)
        return jnp.where(named, rank.astype(jnp.int32), -1), hits

    own_ids = block_of(expert_ids, 0)
    own_slot, _ = slots_of(own_ids)
    normed = normalize(tokens, norm_gain)
    early = own_slot[:, None, :] == jnp.arange(EARLY, dtype=jnp.int32)[:, None]
    chosen = early.astype(jnp.bfloat16).reshape(experts_all * EARLY, tok_count)
    sent = jnp.dot(chosen, normed, preferred_element_type=jnp.float32).astype(jnp.bfloat16)
    arrived = exchange(sent)
    blocks = gather_tp(normed)
    arrived, blocks = lax.optimization_barrier((arrived, blocks))

    masks, masses = [], []
    for at, by in enumerate(OFFSETS):
        ids, weight = block_of(expert_ids, by), block_of(route_weight, by)
        slot, hits = slots_of(ids)
        masses.append(jnp.sum(jnp.where(hits, weight.T[:, None, :], 0.0), axis=0))
        wanted = jnp.full((len(OFFSETS), LATE), -2, jnp.int32)
        wanted = wanted.at[at].set(EARLY + jnp.arange(LATE, dtype=jnp.int32)).reshape(-1)
        masks.append(slot[:, None, :] == wanted[:, None])
    late = jnp.concatenate(masks, axis=2)
    late_rows = experts_all * len(OFFSETS) * LATE
    late_mass = jnp.where(late, jnp.concatenate(masses, axis=1)[:, None, :], 0.0)
    late_mass = late_mass.reshape(late_rows, len(OFFSETS) * tok_count)
    early_mass = jnp.where(early, masses[0][:, None, :], 0.0).reshape(experts_all * EARLY, tok_count)
    late_chosen = late.astype(jnp.bfloat16).reshape(late_rows, len(OFFSETS) * tok_count)
    late_arrived = exchange(select_rows(late_chosen, blocks))

    mid = arrived.shape[0] // 2
    top, bottom = arrived[:mid], arrived[mid:]
    left_top, right_bottom = shift(top, 1), shift(bottom, -1)
    left_bottom, right_top = shift(bottom, 1), shift(top, -1)
    far_top, far_bottom = shift(left_top, 1), shift(right_bottom, -1)
    weights = (exp_gate, exp_up, exp_down)
    own_part, *tiles = expert_streamed(arrived, weights, True)
    left_top, right_bottom, own_part = lax.optimization_barrier((left_top, right_bottom, own_part))
    first = expert_kept([left_top, right_bottom], [mid] * 2, tiles)
    left_bottom, right_top, first = lax.optimization_barrier((left_bottom, right_top, first))
    second = expert_kept([left_bottom, right_top], [mid] * 2, tiles)
    near = send_near(*second)
    far_top, far_bottom, first = lax.optimization_barrier((far_top, far_bottom, first))
    third = expert_kept([far_top, far_bottom], [mid] * 2, tiles)
    via = send_far(*third)
    late_arrived, _ = lax.optimization_barrier((late_arrived, third))
    (late_part,) = expert_streamed(late_arrived, weights, False)
    late_back = exchange(late_part)
    on = send_on(*first, *via)
    summed = jnp.concatenate(near, axis=0).astype(jnp.float32)
    summed = summed + jnp.concatenate(on, axis=0).astype(jnp.float32)
    summed = (summed + own_part.astype(jnp.float32)).astype(jnp.bfloat16)
    back = exchange(summed)

    late_back, _ = lax.optimization_barrier((late_back, summed))
    sums = weigh_rows(late_mass.T, late_back, [tok_count] + [half] * 6)
    token_own, left_top, left_bottom, right_top, right_bottom, far_top, far_bottom = sums
    token_via = send_far(far_top, far_bottom)
    token_near = send_near(left_bottom, right_top)
    token_on = send_on(left_top, right_bottom, *token_via)
    return finish(early_mass.T, back, token_own, token_near + token_on)


def solution(mesh):
    finer = Mesh(mesh.devices.reshape(4, 4, 2, mesh.shape["tp"]), ("ep_0", "ep_1", "ep_2", "tp"))
    return jax.shard_map(
        per_device,
        mesh=finer,
        in_specs=(
            P(EP_TP, None),
            P(),
            P(EP, None),
            P(EP, None),
            P(EP, None, "tp"),
            P(EP, None, "tp"),
            P(EP, "tp", None),
        ),
        out_specs=P(EP_TP, None),
        check_vma=False,
    )
```

```python
import functools

import jax
import jax.numpy as jnp
from jax import lax
from jax.experimental import pallas as pl
from jax.experimental.pallas import tpu as pltpu
from jax.sharding import Mesh
from jax.sharding import PartitionSpec as P


EP = ("ep_0", "ep_1", "ep_2")
EP_TP = ("ep_0", "ep_1", "ep_2", "tp")
CAP = 10
EARLY = 8
LATE = CAP - EARLY
OFFSETS = (0, -1, 1, 2)
UP_TILE = 256
DOWN_TILE = 1024
MIB = 2**20
LANES = 128


norm_eps = 1e-05
VMEM_SPEC = pl.BlockSpec(memory_space=pltpu.VMEM)
SMEM_SPEC = pl.BlockSpec(memory_space=pltpu.SMEM)
HBM_SPEC = pl.BlockSpec(memory_space=pltpu.HBM)


def ones_where(mask):
    return jnp.where(mask, 1.0, 0.0).astype(jnp.bfloat16)


def routed(ids, block, experts_all):
    own = ids[:, pl.ds(pl.multiple_of(block * LANES, LANES), LANES)]
    expert = lax.broadcasted_iota(jnp.int32, (experts_all, LANES), 0)
    return own[0:1] == expert, own[1:2] == expert


def slots_of(hits):
    named = hits[0] | hits[1]
    before = lax.broadcasted_iota(jnp.int32, (LANES, LANES), 0)
    after = lax.broadcasted_iota(jnp.int32, (LANES, LANES), 1)
    rank = jnp.dot(ones_where(named), ones_where(before < after), preferred_element_type=jnp.float32)
    return jnp.where(named, rank, -1.0).astype(jnp.bfloat16)


def per_row(values, rows):
    experts_all = values.shape[0]
    row = lax.broadcasted_iota(jnp.int32, (rows, experts_all), 0) // (rows // experts_all)
    column = lax.broadcasted_iota(jnp.int32, (rows, experts_all), 1)
    return jnp.dot(ones_where(row == column), values, preferred_element_type=jnp.float32)


def early_rows(hits, rows):
    wanted = lax.broadcasted_iota(jnp.int32, (rows, LANES), 0) % EARLY
    return per_row(slots_of(hits), rows) == wanted.astype(jnp.float32)


def late_rows_of(hits, rows, at):
    place_in = lax.broadcasted_iota(jnp.int32, (rows, LANES), 0) % (LATE * len(OFFSETS))
    wanted = jnp.where(place_in // LATE == at, EARLY + place_in % LATE, -2)
    return per_row(slots_of(hits), rows) == wanted.astype(jnp.float32)


def weighted_sum(chosen, hits, route, block, rows):
    weight = route[:, pl.ds(pl.multiple_of(block * LANES, LANES), LANES)]
    mass = jnp.where(hits[0], weight[0:1], 0.0) + jnp.where(hits[1], weight[1:2], 0.0)
    high = mass.astype(jnp.bfloat16)
    low = (mass - high.astype(jnp.float32)).astype(jnp.bfloat16)
    total = None
    for part in (high, low):
        term = jnp.where(chosen, per_row(part, chosen.shape[0]), 0.0).astype(jnp.bfloat16)
        term = lax.dot_general(
            term, rows[...], (((0,), (0,)), ((), ())), preferred_element_type=jnp.float32
        )
        total = term if total is None else total + term
    return total


def block_at(me, by):
    return (me[0] + by + len(OFFSETS)) % len(OFFSETS)


def prepare_kernel(me, tokens, gain, ids, normed, sent):
    experts_all = sent.shape[0] // EARLY
    values = tokens[...].astype(jnp.float32)
    factor = lax.rsqrt(jnp.mean(values * values, axis=-1, keepdims=True) + norm_eps)
    normal = (values * factor * gain[...]).astype(jnp.bfloat16)
    normed[...] = normal
    chosen = ones_where(early_rows(routed(ids, me[0], experts_all), sent.shape[0]))
    sent[...] = jnp.dot(chosen, normal, preferred_element_type=jnp.float32).astype(jnp.bfloat16)


def prepare(tokens, norm_gain, expert_ids, me, experts_all):
    tok_count, d = tokens.shape
    rows = experts_all * EARLY
    return pl.pallas_call(
        prepare_kernel,
        in_specs=[pl.BlockSpec(memory_space=pltpu.SMEM)] + [VMEM_SPEC] * 3,
        out_specs=[VMEM_SPEC] * 2,
        out_shape=[
            jax.ShapeDtypeStruct((tok_count, d), jnp.bfloat16),
            jax.ShapeDtypeStruct((rows, d), jnp.bfloat16),
        ],
        compiler_params=pltpu.CompilerParams(vmem_limit_bytes=16 * MIB),
        cost_estimate=pl.CostEstimate(
            flops=2 * rows * tok_count * d, bytes_accessed=2 * d * (rows + 2 * tok_count), transcendentals=0
        ),
    )(me, *in_hbm(tokens, norm_gain.reshape(1, d), expert_ids))


def in_hbm(*values):
    return tuple(pltpu.with_memory_space_constraint(v, pltpu.HBM) for v in values)


def shift(value, by):
    size = lax.axis_size("tp")
    return lax.ppermute(value, "tp", [(i, (i + by) % size) for i in range(size)])


def exchange(rows):
    ep_size = lax.axis_size(EP)
    tiles = rows.reshape(ep_size, rows.shape[0] // ep_size, rows.shape[1])
    return lax.all_to_all(tiles, EP, 0, 0, tiled=True).reshape(rows.shape)


def gather_tp(rows):
    half = rows.shape[0] // 2
    from_left = shift(rows, 1)
    from_right = shift(rows, -1)
    far_a = shift(from_left[:half], 1)
    far_b = shift(from_right[half:], -1)
    return rows, from_left, from_right, far_a, far_b


def add_kernel(a, b, c, d, left, right):
    left[...] = (a[...].astype(jnp.float32) + b[...].astype(jnp.float32)).astype(left.dtype)
    right[...] = (c[...].astype(jnp.float32) + d[...].astype(jnp.float32)).astype(right.dtype)


def add_pairs(a, b, c, d):
    return pl.pallas_call(
        add_kernel,
        in_specs=[VMEM_SPEC] * 4,
        out_specs=[VMEM_SPEC] * 2,
        out_shape=[jax.ShapeDtypeStruct(v.shape, v.dtype) for v in (a, c)],
        compiler_params=pltpu.CompilerParams(vmem_limit_bytes=12 * MIB),
        cost_estimate=pl.CostEstimate(flops=2 * a.size, bytes_accessed=12 * a.size, transcendentals=0),
    )(a, b, c, d)


def place(target, blocks):
    at = 0
    for b in blocks:
        target[at : at + b.shape[0], :] = b[...]
        at += b.shape[0]


def cut(value, outs, columns=slice(None)):
    at = 0
    for o in outs:
        o[:, columns] = value[at : at + o.shape[0]].astype(o.dtype)
        at += o.shape[0]


def cols(t, width):
    return pl.ds(pl.multiple_of(t * width, width), width)


def expert_rows(rows, hidden, gates, ups, up_tiles, down_tile, outs):
    steps, downs = hidden.shape[1] // UP_TILE, outs[0].shape[1] // DOWN_TILE

    def multiply(t):
        w_gate, w_up = up_tiles(t)
        gate = jnp.dot(rows[...], w_gate[...], preferred_element_type=jnp.float32)
        up = jnp.dot(rows[...], w_up[...], preferred_element_type=jnp.float32)
        return gate, up

    def activate(t):
        gate, up = gates[t % 2], ups[t % 2]
        value = (gate / (1.0 + jnp.exp(-gate)) * up).astype(jnp.bfloat16)
        hidden[:, cols(t, UP_TILE)] = value

    def up_step(t, c):
        gate, up = multiply(t)
        activate(t - 1)
        gates[t % 2] = gate
        ups[t % 2] = up
        return c

    gates[0], ups[0] = multiply(0)
    lax.fori_loop(1, steps, up_step, 0)
    activate(steps - 1)

    def down_step(t, c):
        part = jnp.dot(hidden[...], down_tile(t)[...], preferred_element_type=jnp.float32)
        cut(part, outs, cols(t, DOWN_TILE))
        return c

    lax.fori_loop(0, downs, down_step, 0)


def stream_kernel(n_in, n_out, *refs):
    blocks, (w_gate, w_up, w_down) = refs[:n_in], refs[n_in : n_in + 3]
    outs = refs[n_in + 3 : n_in + 3 + n_out]
    gate_all, up_all, down_all, rows, hidden, gates, ups, sems = refs[n_in + 3 + n_out :]

    def load(kind, t):
        src, dst = ((w_gate, gate_all), (w_up, up_all), (w_down, down_all))[kind]
        at = cols(t, DOWN_TILE if kind == 2 else UP_TILE)
        return pltpu.make_async_copy(src.at[0, :, at], dst.at[:, at], sems.at[kind, t])

    def start_up(t, c):
        load(0, t).start()
        load(1, t).start()
        return c

    def start_down(t, c):
        load(2, t).start()
        return c

    lax.fori_loop(0, gate_all.shape[1] // UP_TILE, start_up, 0)
    lax.fori_loop(0, down_all.shape[1] // DOWN_TILE, start_down, 0)
    place(rows, blocks)

    def up_tiles_of(t):
        load(0, t).wait()
        load(1, t).wait()
        return gate_all.at[:, cols(t, UP_TILE)], up_all.at[:, cols(t, UP_TILE)]

    def down_tile_of(t):
        load(2, t).wait()
        return down_all.at[:, cols(t, DOWN_TILE)]

    expert_rows(rows, hidden, gates, ups, up_tiles_of, down_tile_of, outs)


def kept_kernel(n_in, *refs):
    blocks = refs[:n_in]
    w_gate, w_up, w_down = refs[n_in : n_in + 3]
    outs, rows = refs[n_in + 3 : -1], refs[-1]
    place(rows, blocks)
    gate = jnp.dot(rows[...], w_gate[...], preferred_element_type=jnp.float32)
    up = jnp.dot(rows[...], w_up[...], preferred_element_type=jnp.float32)
    hidden = (gate / (1.0 + jnp.exp(-gate)) * up).astype(jnp.bfloat16)
    cut(jnp.dot(hidden, w_down[...], preferred_element_type=jnp.float32), outs)


def expert_cost(m, d, ff, weights):
    return pl.CostEstimate(
        flops=6 * m * d * ff, bytes_accessed=6 * d * ff * weights + 4 * m * d, transcendentals=m * ff
    )


def row_buffers(m, d, ff):
    return [
        pltpu.VMEM((m, d), jnp.bfloat16),
        pltpu.VMEM((m, ff), jnp.bfloat16),
        pltpu.VMEM((2, m, UP_TILE), jnp.float32),
        pltpu.VMEM((2, m, UP_TILE), jnp.float32),
    ]


def expert_streamed(blocks, sizes, weights, keep):
    d, ff = weights[0].shape[1:]
    m = sum(b.shape[0] for b in blocks)
    steps, downs = ff // UP_TILE, d // DOWN_TILE
    tiles = [
        pltpu.VMEM((d, ff), jnp.bfloat16),
        pltpu.VMEM((d, ff), jnp.bfloat16),
        pltpu.VMEM((ff, d), jnp.bfloat16),
    ]
    return pl.pallas_call(
        functools.partial(stream_kernel, len(blocks), len(sizes)),
        in_specs=[VMEM_SPEC] * len(blocks) + [HBM_SPEC] * 3,
        out_specs=[VMEM_SPEC] * (len(sizes) + (3 if keep else 0)),
        out_shape=[pltpu.HBM((s, d), jnp.bfloat16) for s in sizes] + (tiles if keep else []),
        scratch_shapes=([] if keep else tiles)
        + row_buffers(m, d, ff)
        + [pltpu.SemaphoreType.DMA((3, max(steps, downs)))],
        compiler_params=pltpu.CompilerParams(vmem_limit_bytes=(12 if keep else 34) * MIB),
        cost_estimate=expert_cost(m, d, ff, 1),
    )(*blocks, *in_hbm(*weights))


def expert_kept(blocks, sizes, tiles):
    d, ff = tiles[0].shape
    m = sum(b.shape[0] for b in blocks)
    return pl.pallas_call(
        functools.partial(kept_kernel, len(blocks)),
        in_specs=[VMEM_SPEC] * (len(blocks) + 3),
        out_specs=[VMEM_SPEC] * len(sizes),
        out_shape=[jax.ShapeDtypeStruct((s, d), jnp.bfloat16) for s in sizes],
        scratch_shapes=[pltpu.VMEM((m, d), jnp.bfloat16)],
        compiler_params=pltpu.CompilerParams(vmem_limit_bytes=20 * MIB),
        cost_estimate=expert_cost(m, d, ff, 0),
    )(*blocks, *(pltpu.with_memory_space_constraint(w, pltpu.VMEM) for w in tiles))


def select_kernel(me, ids, *refs):
    blocks, out, rows, chosen = refs[:-3], refs[-3], refs[-2], refs[-1]
    experts_all = out.shape[0] // (LATE * len(OFFSETS))
    place(rows, blocks)
    for at, by in enumerate(OFFSETS):
        hits = routed(ids, block_at(me, by), experts_all)
        chosen[:, at * LANES : (at + 1) * LANES] = ones_where(late_rows_of(hits, out.shape[0], at))
    value = jnp.dot(chosen[...], rows[...], preferred_element_type=jnp.float32)
    out[...] = value.astype(out.dtype)


def select_late(me, expert_ids, blocks, experts_all):
    d = blocks[0].shape[1]
    n, m = experts_all * LATE * len(OFFSETS), LANES * len(OFFSETS)
    return pl.pallas_call(
        select_kernel,
        in_specs=[SMEM_SPEC] + [VMEM_SPEC] * (1 + len(blocks)),
        out_specs=VMEM_SPEC,
        out_shape=jax.ShapeDtypeStruct((n, d), jnp.bfloat16),
        scratch_shapes=[pltpu.VMEM((m, d), jnp.bfloat16), pltpu.VMEM((n, m), jnp.bfloat16)],
        compiler_params=pltpu.CompilerParams(vmem_limit_bytes=16 * MIB),
        cost_estimate=pl.CostEstimate(
            flops=2 * n * m * d, bytes_accessed=2 * d * (n + m), transcendentals=0
        ),
    )(me, expert_ids, *in_hbm(*blocks))


def weigh_kernel(me, ids, route, rows, own, *others):
    experts_all = rows.shape[0] // (LATE * len(OFFSETS))
    for at, by in enumerate(OFFSETS):
        block = block_at(me, by)
        hits = routed(ids, block, experts_all)
        chosen = late_rows_of(hits, rows.shape[0], at)
        value = weighted_sum(chosen, hits, route, block, rows)
        cut(value, [own] if at == 0 else others[2 * at - 2 : 2 * at])


def weigh_late(me, expert_ids, route_weight, rows):
    n, d = rows.shape
    sizes = [LANES] + [LANES // 2] * (2 * len(OFFSETS) - 2)
    return pl.pallas_call(
        weigh_kernel,
        in_specs=[SMEM_SPEC] + [VMEM_SPEC] * 3,
        out_specs=[VMEM_SPEC] * len(sizes),
        out_shape=[pltpu.HBM((s, d), jnp.bfloat16) for s in sizes],
        compiler_params=pltpu.CompilerParams(vmem_limit_bytes=16 * MIB),
        cost_estimate=pl.CostEstimate(
            flops=4 * n * LANES * len(OFFSETS) * d, bytes_accessed=6 * d * n, transcendentals=0
        ),
    )(me, expert_ids, route_weight, rows)


def finish_kernel(me, ids, route, rows, own, near_a, near_b, far_a, far_b, out):
    hits = routed(ids, me[0], rows.shape[0] // EARLY)
    value = weighted_sum(early_rows(hits, rows.shape[0]), hits, route, me[0], rows)
    value = value + own[...].astype(jnp.float32)
    half = out.shape[0] // 2
    top = near_a[...].astype(jnp.float32) + far_a[...].astype(jnp.float32)
    bottom = near_b[...].astype(jnp.float32) + far_b[...].astype(jnp.float32)
    out[:half, :] = (value[:half] + top).astype(out.dtype)
    out[half:, :] = (value[half:] + bottom).astype(out.dtype)


def finish(me, expert_ids, route_weight, rows, own, pieces):
    n, d = rows.shape
    return pl.pallas_call(
        finish_kernel,
        in_specs=[SMEM_SPEC] + [VMEM_SPEC] * 8,
        out_specs=VMEM_SPEC,
        out_shape=jax.ShapeDtypeStruct((LANES, d), jnp.bfloat16),
        compiler_params=pltpu.CompilerParams(vmem_limit_bytes=16 * MIB),
        cost_estimate=pl.CostEstimate(
            flops=4 * n * LANES * d, bytes_accessed=2 * d * (n + 4 * LANES), transcendentals=0
        ),
    )(me, expert_ids, route_weight, rows, own, *pieces)


def send_near(to_left, to_right):
    got_bottom = shift(to_left, -1)
    got_top = shift(to_right, 1)
    return got_top, got_bottom


def send_far(far_top, far_bottom):
    return shift(far_top, -1), shift(far_bottom, 1)


def send_on(to_left, to_right, via_right, via_left):
    left, right = add_pairs(to_left, via_right, to_right, via_left)
    return shift(left, -1), shift(right, 1)


def per_device(tokens, norm_gain, expert_ids, route_weight, exp_gate, exp_up, exp_down):
    experts_all = lax.axis_size(EP)
    me = lax.axis_index("tp").reshape(1)
    ids, route = expert_ids.T, route_weight.T

    normed, sent = prepare(tokens, norm_gain, ids, me, experts_all)
    blocks = gather_tp(normed)
    arrived = exchange(sent)
    arrived, blocks = lax.optimization_barrier((arrived, blocks))

    late_sent = select_late(me, ids, blocks, experts_all)
    late_arrived = exchange(late_sent)

    mid = arrived.shape[0] // 2
    top, bottom = arrived[:mid], arrived[mid:]
    left_top, right_bottom = shift(top, 1), shift(bottom, -1)
    left_bottom, right_top = shift(bottom, 1), shift(top, -1)
    far_top, far_bottom = shift(left_top, 1), shift(right_bottom, -1)
    weights = (exp_gate, exp_up, exp_down)
    *first, gate_tiles, up_tiles, down_tiles = expert_streamed(
        [left_top, right_bottom], [mid] * 2, weights, True
    )
    tiles = (gate_tiles, up_tiles, down_tiles)
    left_bottom, right_top, first = lax.optimization_barrier((left_bottom, right_top, first))
    second = expert_kept([left_bottom, right_top], [mid] * 2, tiles)
    near = send_near(*second)
    far_top, far_bottom, second = lax.optimization_barrier((far_top, far_bottom, second))
    third = expert_kept([far_top, far_bottom], [mid] * 2, tiles)
    via = send_far(*third)
    late_arrived, _ = lax.optimization_barrier((late_arrived, third))
    (late_part,) = expert_streamed([late_arrived], [late_arrived.shape[0]], weights, False)
    late_back = exchange(late_part)
    on = send_on(*first, *via)
    own_rows, _ = lax.optimization_barrier((arrived, (late_part, via)))
    (own_part,) = expert_streamed([own_rows], [2 * mid], weights, False)
    summed = jnp.concatenate(near, axis=0).astype(jnp.float32)
    summed = summed + jnp.concatenate(on, axis=0).astype(jnp.float32)
    summed = (summed + own_part.astype(jnp.float32)).astype(jnp.bfloat16)
    back = exchange(summed)

    late_back, _ = lax.optimization_barrier((late_back, own_part))
    sums = weigh_late(me, ids, route, late_back)
    token_own, left_top, left_bottom, right_top, right_bottom, far_top, far_bottom = sums
    token_via = send_far(far_top, far_bottom)
    token_near = send_near(left_bottom, right_top)
    token_on = send_on(left_top, right_bottom, *token_via)
    return finish(me, ids, route, back, token_own, token_near + token_on)


def solution(mesh):
    finer = Mesh(mesh.devices.reshape(4, 4, 2, mesh.shape["tp"]), ("ep_0", "ep_1", "ep_2", "tp"))
    return jax.shard_map(
        per_device,
        mesh=finer,
        in_specs=(
            P(EP_TP, None),
            P(),
            P(EP, None),
            P(EP, None),
            P(EP, None, "tp"),
            P(EP, None, "tp"),
            P(EP, "tp", None),
        ),
        out_specs=P(EP_TP, None),
        check_vma=False,
    )
```

```python
import functools

import jax
import jax.numpy as jnp
from jax import lax
from jax.experimental import pallas as pl
from jax.experimental.pallas import tpu as pltpu
from jax.sharding import Mesh
from jax.sharding import PartitionSpec as P


EP = ("ep_0", "ep_1", "ep_2")
EP_TP = ("ep_0", "ep_1", "ep_2", "tp")
CAP = 10
EARLY = 8
LATE = CAP - EARLY
OFFSETS = (0, -1, 1, 2)
UP_TILE = 256
DOWN_TILE = 1024
MIB = 2**20
LANES = 128


norm_eps = 1e-05
VMEM_SPEC = pl.BlockSpec(memory_space=pltpu.VMEM)
SMEM_SPEC = pl.BlockSpec(memory_space=pltpu.SMEM)
HBM_SPEC = pl.BlockSpec(memory_space=pltpu.HBM)


def ones_where(mask):
    return jnp.where(mask, 1.0, 0.0).astype(jnp.bfloat16)


def routed(ids, block, experts_all):
    own = ids[:, pl.ds(pl.multiple_of(block * LANES, LANES), LANES)]
    expert = lax.broadcasted_iota(jnp.int32, (experts_all, LANES), 0)
    return own[0:1] == expert, own[1:2] == expert


def slots_of(hits):
    named = hits[0] | hits[1]
    before = lax.broadcasted_iota(jnp.int32, (LANES, LANES), 0)
    after = lax.broadcasted_iota(jnp.int32, (LANES, LANES), 1)
    rank = jnp.dot(ones_where(named), ones_where(before < after), preferred_element_type=jnp.float32)
    return jnp.where(named, rank, -1.0).astype(jnp.bfloat16)


def per_row(values, rows):
    experts_all = values.shape[0]
    row = lax.broadcasted_iota(jnp.int32, (rows, experts_all), 0) // (rows // experts_all)
    column = lax.broadcasted_iota(jnp.int32, (rows, experts_all), 1)
    return jnp.dot(ones_where(row == column), values, preferred_element_type=jnp.float32)


def early_rows(hits, rows):
    wanted = lax.broadcasted_iota(jnp.int32, (rows, LANES), 0) % EARLY
    return per_row(slots_of(hits), rows) == wanted.astype(jnp.float32)


def late_rows_of(hits, rows, at):
    place_in = lax.broadcasted_iota(jnp.int32, (rows, LANES), 0) % (LATE * len(OFFSETS))
    wanted = jnp.where(place_in // LATE == at, EARLY + place_in % LATE, -2)
    return per_row(slots_of(hits), rows) == wanted.astype(jnp.float32)


def weights_of(chosen, hits, route, block):
    weight = route[:, pl.ds(pl.multiple_of(block * LANES, LANES), LANES)]
    mass = jnp.where(hits[0], weight[0:1], 0.0) + jnp.where(hits[1], weight[1:2], 0.0)
    high = mass.astype(jnp.bfloat16)
    low = (mass - high.astype(jnp.float32)).astype(jnp.bfloat16)
    terms = (jnp.where(chosen, per_row(t, chosen.shape[0]), 0.0) for t in (high, low))
    return tuple(t.T.astype(jnp.bfloat16) for t in terms)


def weighted_sum(high, low, rows):
    value = jnp.dot(high, rows, preferred_element_type=jnp.float32)
    return value + jnp.dot(low, rows, preferred_element_type=jnp.float32)


def block_at(me, by):
    return (me[0] + by + len(OFFSETS)) % len(OFFSETS)


def prepare_kernel(me, tokens, gain, ids, normed, sent):
    experts_all = sent.shape[0] // EARLY
    values = tokens[...].astype(jnp.float32)
    factor = lax.rsqrt(jnp.mean(values * values, axis=-1, keepdims=True) + norm_eps)
    normal = (values * factor * gain[...]).astype(jnp.bfloat16)
    normed[...] = normal
    chosen = ones_where(early_rows(routed(ids, me[0], experts_all), sent.shape[0]))
    sent[...] = jnp.dot(chosen, normal, preferred_element_type=jnp.float32).astype(jnp.bfloat16)


def prepare(tokens, norm_gain, expert_ids, me, experts_all):
    tok_count, d = tokens.shape
    rows = experts_all * EARLY
    return pl.pallas_call(
        prepare_kernel,
        in_specs=[pl.BlockSpec(memory_space=pltpu.SMEM)] + [VMEM_SPEC] * 3,
        out_specs=[VMEM_SPEC] * 2,
        out_shape=[
            jax.ShapeDtypeStruct((tok_count, d), jnp.bfloat16),
            jax.ShapeDtypeStruct((rows, d), jnp.bfloat16),
        ],
        compiler_params=pltpu.CompilerParams(vmem_limit_bytes=16 * MIB),
        cost_estimate=pl.CostEstimate(
            flops=2 * rows * tok_count * d, bytes_accessed=2 * d * (rows + 2 * tok_count), transcendentals=0
        ),
    )(me, *in_hbm(tokens, norm_gain.reshape(1, d), expert_ids))


def in_hbm(*values):
    return tuple(pltpu.with_memory_space_constraint(v, pltpu.HBM) for v in values)


def shift(value, by):
    size = lax.axis_size("tp")
    return lax.ppermute(value, "tp", [(i, (i + by) % size) for i in range(size)])


def exchange(rows):
    ep_size = lax.axis_size(EP)
    tiles = rows.reshape(ep_size, rows.shape[0] // ep_size, rows.shape[1])
    return lax.all_to_all(tiles, EP, 0, 0, tiled=True).reshape(rows.shape)


def gather_tp(rows):
    half = rows.shape[0] // 2
    from_left = shift(rows, 1)
    from_right = shift(rows, -1)
    far_a = shift(from_left[:half], 1)
    far_b = shift(from_right[half:], -1)
    return rows, from_left, from_right, far_a, far_b


def add_kernel(a, b, c, d, left, right):
    left[...] = (a[...].astype(jnp.float32) + b[...].astype(jnp.float32)).astype(left.dtype)
    right[...] = (c[...].astype(jnp.float32) + d[...].astype(jnp.float32)).astype(right.dtype)


def add_pairs(a, b, c, d):
    return pl.pallas_call(
        add_kernel,
        in_specs=[VMEM_SPEC] * 4,
        out_specs=[VMEM_SPEC] * 2,
        out_shape=[jax.ShapeDtypeStruct(v.shape, v.dtype) for v in (a, c)],
        compiler_params=pltpu.CompilerParams(vmem_limit_bytes=12 * MIB),
        cost_estimate=pl.CostEstimate(flops=2 * a.size, bytes_accessed=12 * a.size, transcendentals=0),
    )(a, b, c, d)


def place(target, blocks):
    at = 0
    for b in blocks:
        target[at : at + b.shape[0], :] = b[...]
        at += b.shape[0]


def cut(value, outs, columns=slice(None)):
    at = 0
    for o in outs:
        o[:, columns] = value[at : at + o.shape[0]].astype(o.dtype)
        at += o.shape[0]


def cols(t, width):
    return pl.ds(pl.multiple_of(t * width, width), width)


def expert_rows(rows, hidden, gates, ups, up_tiles, down_tile, outs):
    steps, downs = hidden.shape[1] // UP_TILE, outs[0].shape[1] // DOWN_TILE

    def multiply(t):
        w_gate, w_up = up_tiles(t)
        gate = jnp.dot(rows[...], w_gate[...], preferred_element_type=jnp.float32)
        up = jnp.dot(rows[...], w_up[...], preferred_element_type=jnp.float32)
        return gate, up

    def activate(t):
        gate, up = gates[t % 2], ups[t % 2]
        value = (gate / (1.0 + jnp.exp(-gate)) * up).astype(jnp.bfloat16)
        hidden[:, cols(t, UP_TILE)] = value

    def up_step(t, c):
        gate, up = multiply(t)
        activate(t - 1)
        gates[t % 2] = gate
        ups[t % 2] = up
        return c

    gates[0], ups[0] = multiply(0)
    lax.fori_loop(1, steps, up_step, 0)
    activate(steps - 1)

    def down_step(t, c):
        part = jnp.dot(hidden[...], down_tile(t)[...], preferred_element_type=jnp.float32)
        cut(part, outs, cols(t, DOWN_TILE))
        return c

    lax.fori_loop(0, downs, down_step, 0)


def stream_kernel(n_in, n_out, *refs):
    blocks, (w_gate, w_up, w_down) = refs[:n_in], refs[n_in : n_in + 3]
    outs = refs[n_in + 3 : n_in + 3 + n_out]
    gate_all, up_all, down_all, rows, hidden, gates, ups, sems = refs[n_in + 3 + n_out :]

    def load(kind, t):
        src, dst = ((w_gate, gate_all), (w_up, up_all), (w_down, down_all))[kind]
        at = cols(t, DOWN_TILE if kind == 2 else UP_TILE)
        return pltpu.make_async_copy(src.at[0, :, at], dst.at[:, at], sems.at[kind, t])

    def start_up(t, c):
        load(0, t).start()
        load(1, t).start()
        return c

    def start_down(t, c):
        load(2, t).start()
        return c

    lax.fori_loop(0, gate_all.shape[1] // UP_TILE, start_up, 0)
    lax.fori_loop(0, down_all.shape[1] // DOWN_TILE, start_down, 0)
    place(rows, blocks)

    def up_tiles_of(t):
        load(0, t).wait()
        load(1, t).wait()
        return gate_all.at[:, cols(t, UP_TILE)], up_all.at[:, cols(t, UP_TILE)]

    def down_tile_of(t):
        load(2, t).wait()
        return down_all.at[:, cols(t, DOWN_TILE)]

    expert_rows(rows, hidden, gates, ups, up_tiles_of, down_tile_of, outs)


def kept_kernel(n_in, *refs):
    blocks = refs[:n_in]
    w_gate, w_up, w_down = refs[n_in : n_in + 3]
    outs, rows = refs[n_in + 3 : -1], refs[-1]
    place(rows, blocks)
    gate = jnp.dot(rows[...], w_gate[...], preferred_element_type=jnp.float32)
    up = jnp.dot(rows[...], w_up[...], preferred_element_type=jnp.float32)
    hidden = (gate / (1.0 + jnp.exp(-gate)) * up).astype(jnp.bfloat16)
    cut(jnp.dot(hidden, w_down[...], preferred_element_type=jnp.float32), outs)


def expert_cost(m, d, ff, weights):
    return pl.CostEstimate(
        flops=6 * m * d * ff, bytes_accessed=6 * d * ff * weights + 4 * m * d, transcendentals=m * ff
    )


def row_buffers(m, d, ff):
    return [
        pltpu.VMEM((m, d), jnp.bfloat16),
        pltpu.VMEM((m, ff), jnp.bfloat16),
        pltpu.VMEM((2, m, UP_TILE), jnp.float32),
        pltpu.VMEM((2, m, UP_TILE), jnp.float32),
    ]


def expert_streamed(blocks, sizes, weights, keep):
    d, ff = weights[0].shape[1:]
    m = sum(b.shape[0] for b in blocks)
    steps, downs = ff // UP_TILE, d // DOWN_TILE
    tiles = [
        pltpu.VMEM((d, ff), jnp.bfloat16),
        pltpu.VMEM((d, ff), jnp.bfloat16),
        pltpu.VMEM((ff, d), jnp.bfloat16),
    ]
    return pl.pallas_call(
        functools.partial(stream_kernel, len(blocks), len(sizes)),
        in_specs=[VMEM_SPEC] * len(blocks) + [HBM_SPEC] * 3,
        out_specs=[VMEM_SPEC] * (len(sizes) + (3 if keep else 0)),
        out_shape=[pltpu.HBM((s, d), jnp.bfloat16) for s in sizes] + (tiles if keep else []),
        scratch_shapes=([] if keep else tiles)
        + row_buffers(m, d, ff)
        + [pltpu.SemaphoreType.DMA((3, max(steps, downs)))],
        compiler_params=pltpu.CompilerParams(vmem_limit_bytes=(12 if keep else 34) * MIB),
        cost_estimate=expert_cost(m, d, ff, 1),
    )(*blocks, *in_hbm(*weights))


def expert_kept(blocks, sizes, tiles):
    d, ff = tiles[0].shape
    m = sum(b.shape[0] for b in blocks)
    return pl.pallas_call(
        functools.partial(kept_kernel, len(blocks)),
        in_specs=[VMEM_SPEC] * (len(blocks) + 3),
        out_specs=[VMEM_SPEC] * len(sizes),
        out_shape=[jax.ShapeDtypeStruct((s, d), jnp.bfloat16) for s in sizes],
        scratch_shapes=[pltpu.VMEM((m, d), jnp.bfloat16)],
        compiler_params=pltpu.CompilerParams(vmem_limit_bytes=20 * MIB),
        cost_estimate=expert_cost(m, d, ff, 0),
    )(*blocks, *(pltpu.with_memory_space_constraint(w, pltpu.VMEM) for w in tiles))


def route_kernel(me, ids, route, late, late_high, late_low, high, low):
    rows = late.shape[0]
    experts_all = rows // (LATE * len(OFFSETS))
    for at, by in enumerate(OFFSETS):
        block = block_at(me, by)
        hits = routed(ids, block, experts_all)
        chosen = late_rows_of(hits, rows, at)
        tokens = pl.ds(at * LANES, LANES)
        late[:, tokens] = ones_where(chosen)
        late_high[tokens, :], late_low[tokens, :] = weights_of(chosen, hits, route, block)
        if at == 0:
            chosen = early_rows(hits, high.shape[1])
            high[...], low[...] = weights_of(chosen, hits, route, block)


def route_tables(me, expert_ids, route_weight, experts_all):
    rows, tokens = experts_all * LATE * len(OFFSETS), LANES * len(OFFSETS)
    shapes = [(rows, tokens)] + [(tokens, rows)] * 2 + [(LANES, experts_all * EARLY)] * 2
    return pl.pallas_call(
        route_kernel,
        in_specs=[SMEM_SPEC] + [VMEM_SPEC] * 2,
        out_specs=[VMEM_SPEC] * len(shapes),
        out_shape=[pltpu.HBM(s, jnp.bfloat16) for s in shapes],
        compiler_params=pltpu.CompilerParams(vmem_limit_bytes=16 * MIB),
        cost_estimate=pl.CostEstimate(
            flops=4 * 10**9, bytes_accessed=6 * rows * tokens, transcendentals=0
        ),
    )(me, *in_hbm(expert_ids, route_weight))


def select_kernel(chosen, *refs):
    blocks, out, rows = refs[:-2], refs[-2], refs[-1]
    place(rows, blocks)
    value = jnp.dot(chosen[...], rows[...], preferred_element_type=jnp.float32)
    out[...] = value.astype(out.dtype)


def select_late(chosen, blocks):
    d = blocks[0].shape[1]
    n, m = chosen.shape
    return pl.pallas_call(
        select_kernel,
        in_specs=[VMEM_SPEC] * (1 + len(blocks)),
        out_specs=VMEM_SPEC,
        out_shape=pltpu.HBM((n, d), jnp.bfloat16),
        scratch_shapes=[pltpu.VMEM((m, d), jnp.bfloat16)],
        compiler_params=pltpu.CompilerParams(vmem_limit_bytes=16 * MIB),
        cost_estimate=pl.CostEstimate(
            flops=2 * n * m * d, bytes_accessed=2 * d * (n + m), transcendentals=0
        ),
    )(*in_hbm(chosen, *blocks))


def weigh_kernel(high, low, rows, *outs):
    cut(weighted_sum(high[...], low[...], rows[...]), outs)


def weigh_late(high, low, rows):
    n, d = rows.shape
    sizes = [LANES] + [LANES // 2] * (2 * len(OFFSETS) - 2)
    return pl.pallas_call(
        weigh_kernel,
        in_specs=[VMEM_SPEC] * 3,
        out_specs=[VMEM_SPEC] * len(sizes),
        out_shape=[pltpu.HBM((s, d), jnp.bfloat16) for s in sizes],
        compiler_params=pltpu.CompilerParams(vmem_limit_bytes=16 * MIB),
        cost_estimate=pl.CostEstimate(
            flops=4 * n * LANES * len(OFFSETS) * d, bytes_accessed=6 * d * n, transcendentals=0
        ),
    )(high, low, rows)


def finish_kernel(high, low, rows, own, near_a, near_b, far_a, far_b, out):
    value = weighted_sum(high[...], low[...], rows[...])
    value = value + own[...].astype(jnp.float32)
    half = out.shape[0] // 2
    top = near_a[...].astype(jnp.float32) + far_a[...].astype(jnp.float32)
    bottom = near_b[...].astype(jnp.float32) + far_b[...].astype(jnp.float32)
    out[:half, :] = (value[:half] + top).astype(out.dtype)
    out[half:, :] = (value[half:] + bottom).astype(out.dtype)


def finish(high, low, rows, own, pieces):
    n, d = rows.shape
    return pl.pallas_call(
        finish_kernel,
        in_specs=[VMEM_SPEC] * 8,
        out_specs=VMEM_SPEC,
        out_shape=jax.ShapeDtypeStruct((LANES, d), jnp.bfloat16),
        compiler_params=pltpu.CompilerParams(vmem_limit_bytes=16 * MIB),
        cost_estimate=pl.CostEstimate(
            flops=4 * n * LANES * d, bytes_accessed=2 * d * (n + 4 * LANES), transcendentals=0
        ),
    )(high, low, rows, own, *pieces)


def send_near(to_left, to_right):
    got_bottom = shift(to_left, -1)
    got_top = shift(to_right, 1)
    return got_top, got_bottom


def send_far(far_top, far_bottom):
    return shift(far_top, -1), shift(far_bottom, 1)


def send_on(to_left, to_right, via_right, via_left):
    left, right = add_pairs(to_left, via_right, to_right, via_left)
    return shift(left, -1), shift(right, 1)


def per_device(tokens, norm_gain, expert_ids, route_weight, exp_gate, exp_up, exp_down):
    experts_all = lax.axis_size(EP)
    me = lax.axis_index("tp").reshape(1)
    ids, route = expert_ids.T, route_weight.T

    normed, sent = prepare(tokens, norm_gain, ids, me, experts_all)
    blocks = gather_tp(normed)
    arrived = exchange(sent)
    arrived, blocks = lax.optimization_barrier((arrived, blocks))

    late_chosen, late_high, late_low, high, low = route_tables(me, ids, route, experts_all)
    late_sent = select_late(late_chosen, blocks)
    late_arrived = exchange(late_sent)

    mid = arrived.shape[0] // 2
    top, bottom = arrived[:mid], arrived[mid:]
    left_top, right_bottom = shift(top, 1), shift(bottom, -1)
    left_bottom, right_top = shift(bottom, 1), shift(top, -1)
    far_top, far_bottom = shift(left_top, 1), shift(right_bottom, -1)
    weights = (exp_gate, exp_up, exp_down)
    *first, gate_tiles, up_tiles, down_tiles = expert_streamed(
        [left_top, right_bottom], [mid] * 2, weights, True
    )
    tiles = (gate_tiles, up_tiles, down_tiles)
    left_bottom, right_top, first = lax.optimization_barrier((left_bottom, right_top, first))
    second = expert_kept([left_bottom, right_top], [mid] * 2, tiles)
    near = send_near(*second)
    far_top, far_bottom, second = lax.optimization_barrier((far_top, far_bottom, second))
    third = expert_kept([far_top, far_bottom], [mid] * 2, tiles)
    via = send_far(*third)
    late_arrived, _ = lax.optimization_barrier((late_arrived, third))
    (late_part,) = expert_streamed([late_arrived], [late_arrived.shape[0]], weights, False)
    late_back = exchange(late_part)
    on = send_on(*first, *via)
    own_rows, _ = lax.optimization_barrier((arrived, (late_part, via)))
    (own_part,) = expert_streamed([own_rows], [2 * mid], weights, False)
    summed = jnp.concatenate(near, axis=0).astype(jnp.float32)
    summed = summed + jnp.concatenate(on, axis=0).astype(jnp.float32)
    summed = (summed + own_part.astype(jnp.float32)).astype(jnp.bfloat16)
    back = exchange(summed)

    late_back, _ = lax.optimization_barrier((late_back, own_part))
    sums = weigh_late(late_high, late_low, late_back)
    token_own, left_top, left_bottom, right_top, right_bottom, far_top, far_bottom = sums
    token_via = send_far(far_top, far_bottom)
    token_near = send_near(left_bottom, right_top)
    token_on = send_on(left_top, right_bottom, *token_via)
    return finish(high, low, back, token_own, token_near + token_on)


def solution(mesh):
    finer = Mesh(mesh.devices.reshape(4, 4, 2, mesh.shape["tp"]), ("ep_0", "ep_1", "ep_2", "tp"))
    return jax.shard_map(
        per_device,
        mesh=finer,
        in_specs=(
            P(EP_TP, None),
            P(),
            P(EP, None),
            P(EP, None),
            P(EP, None, "tp"),
            P(EP, None, "tp"),
            P(EP, "tp", None),
        ),
        out_specs=P(EP_TP, None),
        check_vma=False,
    )
```

```python
import functools

import jax
import jax.numpy as jnp
from jax import lax
from jax.experimental import pallas as pl
from jax.experimental.pallas import tpu as pltpu
from jax.sharding import Mesh
from jax.sharding import PartitionSpec as P


EP = ("ep_0", "ep_1", "ep_2")
EP_TP = ("ep_0", "ep_1", "ep_2", "tp")
CAP = 10
EARLY = 8
LATE = CAP - EARLY
OFFSETS = (0, -1, 1, 2)
UP_TILE = 256
DOWN_TILE = 1024
MIB = 2**20
LANES = 128


norm_eps = 1e-05
VMEM_SPEC = pl.BlockSpec(memory_space=pltpu.VMEM)
SMEM_SPEC = pl.BlockSpec(memory_space=pltpu.SMEM)
HBM_SPEC = pl.BlockSpec(memory_space=pltpu.HBM)


def ones_where(mask):
    return jnp.where(mask, 1.0, 0.0).astype(jnp.bfloat16)


def routed(ids, block, experts_all):
    own = ids[:, pl.ds(pl.multiple_of(block * LANES, LANES), LANES)]
    expert = lax.broadcasted_iota(jnp.int32, (experts_all, LANES), 0)
    return own[0:1] == expert, own[1:2] == expert


def slots_of(hits):
    named = hits[0] | hits[1]
    before = lax.broadcasted_iota(jnp.int32, (LANES, LANES), 0)
    after = lax.broadcasted_iota(jnp.int32, (LANES, LANES), 1)
    rank = jnp.dot(ones_where(named), ones_where(before < after), preferred_element_type=jnp.float32)
    return jnp.where(named, rank, -1.0).astype(jnp.bfloat16)


def per_row(values, rows):
    experts_all = values.shape[0]
    row = lax.broadcasted_iota(jnp.int32, (rows, experts_all), 0) // (rows // experts_all)
    column = lax.broadcasted_iota(jnp.int32, (rows, experts_all), 1)
    return jnp.dot(ones_where(row == column), values, preferred_element_type=jnp.float32)


def early_rows(hits, rows):
    wanted = lax.broadcasted_iota(jnp.int32, (rows, LANES), 0) % EARLY
    return per_row(slots_of(hits), rows) == wanted.astype(jnp.float32)


def late_rows_of(hits, rows, at):
    place_in = lax.broadcasted_iota(jnp.int32, (rows, LANES), 0) % (LATE * len(OFFSETS))
    wanted = jnp.where(place_in // LATE == at, EARLY + place_in % LATE, -2)
    return per_row(slots_of(hits), rows) == wanted.astype(jnp.float32)


def weights_of(chosen, hits, route, block):
    weight = route[:, pl.ds(pl.multiple_of(block * LANES, LANES), LANES)]
    mass = jnp.where(hits[0], weight[0:1], 0.0) + jnp.where(hits[1], weight[1:2], 0.0)
    high = mass.astype(jnp.bfloat16)
    low = (mass - high.astype(jnp.float32)).astype(jnp.bfloat16)
    terms = (jnp.where(chosen, per_row(t, chosen.shape[0]), 0.0) for t in (high, low))
    return tuple(t.T.astype(jnp.bfloat16) for t in terms)


def weighted_sum(high, low, rows):
    value = jnp.dot(high, rows, preferred_element_type=jnp.float32)
    return value + jnp.dot(low, rows, preferred_element_type=jnp.float32)


def block_at(me, by):
    return (me[0] + by + len(OFFSETS)) % len(OFFSETS)


def prepare_kernel(me, tokens, gain, ids, normed, sent):
    experts_all = sent.shape[0] // EARLY
    values = tokens[...].astype(jnp.float32)
    factor = lax.rsqrt(jnp.mean(values * values, axis=-1, keepdims=True) + norm_eps)
    normal = (values * factor * gain[...]).astype(jnp.bfloat16)
    normed[...] = normal
    chosen = ones_where(early_rows(routed(ids, me[0], experts_all), sent.shape[0]))
    sent[...] = jnp.dot(chosen, normal, preferred_element_type=jnp.float32).astype(jnp.bfloat16)


def prepare(tokens, norm_gain, expert_ids, me, experts_all):
    tok_count, d = tokens.shape
    rows = experts_all * EARLY
    return pl.pallas_call(
        prepare_kernel,
        in_specs=[pl.BlockSpec(memory_space=pltpu.SMEM)] + [VMEM_SPEC] * 3,
        out_specs=[VMEM_SPEC] * 2,
        out_shape=[
            jax.ShapeDtypeStruct((tok_count, d), jnp.bfloat16),
            jax.ShapeDtypeStruct((rows, d), jnp.bfloat16),
        ],
        compiler_params=pltpu.CompilerParams(vmem_limit_bytes=16 * MIB),
        cost_estimate=pl.CostEstimate(
            flops=2 * rows * tok_count * d, bytes_accessed=2 * d * (rows + 2 * tok_count), transcendentals=0
        ),
    )(me, *in_hbm(tokens, norm_gain.reshape(1, d), expert_ids))


def in_hbm(*values):
    return tuple(pltpu.with_memory_space_constraint(v, pltpu.HBM) for v in values)


def shift(value, by):
    size = lax.axis_size("tp")
    return lax.ppermute(value, "tp", [(i, (i + by) % size) for i in range(size)])


def exchange(rows):
    ep_size = lax.axis_size(EP)
    tiles = rows.reshape(ep_size, rows.shape[0] // ep_size, rows.shape[1])
    return lax.all_to_all(tiles, EP, 0, 0, tiled=True).reshape(rows.shape)


def gather_tp(rows):
    half = rows.shape[0] // 2
    from_left = shift(rows, 1)
    from_right = shift(rows, -1)
    far_a = shift(from_left[:half], 1)
    far_b = shift(from_right[half:], -1)
    return rows, from_left, from_right, far_a, far_b


def add_kernel(a, b, c, d, left, right):
    left[...] = (a[...].astype(jnp.float32) + b[...].astype(jnp.float32)).astype(left.dtype)
    right[...] = (c[...].astype(jnp.float32) + d[...].astype(jnp.float32)).astype(right.dtype)


def add_pairs(a, b, c, d):
    return pl.pallas_call(
        add_kernel,
        in_specs=[VMEM_SPEC] * 4,
        out_specs=[VMEM_SPEC] * 2,
        out_shape=[jax.ShapeDtypeStruct(v.shape, v.dtype) for v in (a, c)],
        compiler_params=pltpu.CompilerParams(vmem_limit_bytes=12 * MIB),
        cost_estimate=pl.CostEstimate(flops=2 * a.size, bytes_accessed=12 * a.size, transcendentals=0),
    )(*in_hbm(a, b, c, d))


def place(target, blocks):
    at = 0
    for b in blocks:
        target[at : at + b.shape[0], :] = b[...]
        at += b.shape[0]


def cut(value, outs, columns=slice(None)):
    at = 0
    for o in outs:
        o[:, columns] = value[at : at + o.shape[0]].astype(o.dtype)
        at += o.shape[0]


def cols(t, width):
    return pl.ds(pl.multiple_of(t * width, width), width)


def expert_rows(rows, hidden, gates, ups, up_tiles, down_tile, outs):
    steps, downs = hidden.shape[1] // UP_TILE, outs[0].shape[1] // DOWN_TILE

    def multiply(t):
        w_gate, w_up = up_tiles(t)
        gate = jnp.dot(rows[...], w_gate[...], preferred_element_type=jnp.float32)
        up = jnp.dot(rows[...], w_up[...], preferred_element_type=jnp.float32)
        return gate, up

    def activate(t):
        gate, up = gates[t % 2], ups[t % 2]
        value = (gate / (1.0 + jnp.exp(-gate)) * up).astype(jnp.bfloat16)
        hidden[:, cols(t, UP_TILE)] = value

    def up_step(t, c):
        gate, up = multiply(t)
        activate(t - 1)
        gates[t % 2] = gate
        ups[t % 2] = up
        return c

    gates[0], ups[0] = multiply(0)
    lax.fori_loop(1, steps, up_step, 0)
    activate(steps - 1)

    def down_step(t, c):
        part = jnp.dot(hidden[...], down_tile(t)[...], preferred_element_type=jnp.float32)
        cut(part, outs, cols(t, DOWN_TILE))
        return c

    lax.fori_loop(0, downs, down_step, 0)


def stream_kernel(n_in, n_out, *refs):
    blocks, (w_gate, w_up, w_down) = refs[:n_in], refs[n_in : n_in + 3]
    outs = refs[n_in + 3 : n_in + 3 + n_out]
    gate_all, up_all, down_all, rows, hidden, gates, ups, sems = refs[n_in + 3 + n_out :]

    def load(kind, t):
        src, dst = ((w_gate, gate_all), (w_up, up_all), (w_down, down_all))[kind]
        at = cols(t, DOWN_TILE if kind == 2 else UP_TILE)
        return pltpu.make_async_copy(src.at[0, :, at], dst.at[:, at], sems.at[kind, t])

    def start_up(t, c):
        load(0, t).start()
        load(1, t).start()
        return c

    def start_down(t, c):
        load(2, t).start()
        return c

    lax.fori_loop(0, gate_all.shape[1] // UP_TILE, start_up, 0)
    lax.fori_loop(0, down_all.shape[1] // DOWN_TILE, start_down, 0)
    place(rows, blocks)

    def up_tiles_of(t):
        load(0, t).wait()
        load(1, t).wait()
        return gate_all.at[:, cols(t, UP_TILE)], up_all.at[:, cols(t, UP_TILE)]

    def down_tile_of(t):
        load(2, t).wait()
        return down_all.at[:, cols(t, DOWN_TILE)]

    expert_rows(rows, hidden, gates, ups, up_tiles_of, down_tile_of, outs)


def kept_kernel(n_in, *refs):
    blocks = refs[:n_in]
    w_gate, w_up, w_down = refs[n_in : n_in + 3]
    outs, rows = refs[n_in + 3 : -1], refs[-1]
    place(rows, blocks)
    gate = jnp.dot(rows[...], w_gate[...], preferred_element_type=jnp.float32)
    up = jnp.dot(rows[...], w_up[...], preferred_element_type=jnp.float32)
    hidden = (gate / (1.0 + jnp.exp(-gate)) * up).astype(jnp.bfloat16)
    cut(jnp.dot(hidden, w_down[...], preferred_element_type=jnp.float32), outs)


def expert_cost(m, d, ff, weights):
    return pl.CostEstimate(
        flops=6 * m * d * ff, bytes_accessed=6 * d * ff * weights + 4 * m * d, transcendentals=m * ff
    )


def row_buffers(m, d, ff):
    return [
        pltpu.VMEM((m, d), jnp.bfloat16),
        pltpu.VMEM((m, ff), jnp.bfloat16),
        pltpu.VMEM((2, m, UP_TILE), jnp.float32),
        pltpu.VMEM((2, m, UP_TILE), jnp.float32),
    ]


def expert_streamed(blocks, sizes, weights, keep):
    d, ff = weights[0].shape[1:]
    m = sum(b.shape[0] for b in blocks)
    steps, downs = ff // UP_TILE, d // DOWN_TILE
    tiles = [
        pltpu.VMEM((d, ff), jnp.bfloat16),
        pltpu.VMEM((d, ff), jnp.bfloat16),
        pltpu.VMEM((ff, d), jnp.bfloat16),
    ]
    return pl.pallas_call(
        functools.partial(stream_kernel, len(blocks), len(sizes)),
        in_specs=[VMEM_SPEC] * len(blocks) + [HBM_SPEC] * 3,
        out_specs=[VMEM_SPEC] * (len(sizes) + (3 if keep else 0)),
        out_shape=[pltpu.HBM((s, d), jnp.bfloat16) for s in sizes] + (tiles if keep else []),
        scratch_shapes=([] if keep else tiles)
        + row_buffers(m, d, ff)
        + [pltpu.SemaphoreType.DMA((3, max(steps, downs)))],
        compiler_params=pltpu.CompilerParams(vmem_limit_bytes=(12 if keep else 34) * MIB),
        cost_estimate=expert_cost(m, d, ff, 1),
    )(*blocks, *in_hbm(*weights))


def expert_kept(blocks, sizes, tiles):
    d, ff = tiles[0].shape
    m = sum(b.shape[0] for b in blocks)
    return pl.pallas_call(
        functools.partial(kept_kernel, len(blocks)),
        in_specs=[VMEM_SPEC] * (len(blocks) + 3),
        out_specs=[VMEM_SPEC] * len(sizes),
        out_shape=[jax.ShapeDtypeStruct((s, d), jnp.bfloat16) for s in sizes],
        scratch_shapes=[pltpu.VMEM((m, d), jnp.bfloat16)],
        compiler_params=pltpu.CompilerParams(vmem_limit_bytes=20 * MIB),
        cost_estimate=expert_cost(m, d, ff, 0),
    )(*blocks, *(pltpu.with_memory_space_constraint(w, pltpu.VMEM) for w in tiles))


def route_kernel(me, ids, route, late, late_high, late_low, high, low):
    rows = late.shape[0]
    experts_all = rows // (LATE * len(OFFSETS))
    for at, by in enumerate(OFFSETS):
        block = block_at(me, by)
        hits = routed(ids, block, experts_all)
        chosen = late_rows_of(hits, rows, at)
        tokens = pl.ds(at * LANES, LANES)
        late[:, tokens] = ones_where(chosen)
        late_high[tokens, :], late_low[tokens, :] = weights_of(chosen, hits, route, block)
        if at == 0:
            chosen = early_rows(hits, high.shape[1])
            high[...], low[...] = weights_of(chosen, hits, route, block)


def route_tables(me, expert_ids, route_weight, experts_all):
    rows, tokens = experts_all * LATE * len(OFFSETS), LANES * len(OFFSETS)
    shapes = [(rows, tokens)] + [(tokens, rows)] * 2 + [(LANES, experts_all * EARLY)] * 2
    return pl.pallas_call(
        route_kernel,
        in_specs=[SMEM_SPEC] + [VMEM_SPEC] * 2,
        out_specs=[VMEM_SPEC] * len(shapes),
        out_shape=[pltpu.HBM(s, jnp.bfloat16) for s in shapes],
        compiler_params=pltpu.CompilerParams(vmem_limit_bytes=16 * MIB),
        cost_estimate=pl.CostEstimate(
            flops=4 * 10**9, bytes_accessed=6 * rows * tokens, transcendentals=0
        ),
    )(me, *in_hbm(expert_ids, route_weight))


def select_kernel(chosen, *refs):
    blocks, out, rows = refs[:-2], refs[-2], refs[-1]
    place(rows, blocks)
    value = jnp.dot(chosen[...], rows[...], preferred_element_type=jnp.float32)
    out[...] = value.astype(out.dtype)


def select_late(chosen, blocks):
    d = blocks[0].shape[1]
    n, m = chosen.shape
    return pl.pallas_call(
        select_kernel,
        in_specs=[VMEM_SPEC] * (1 + len(blocks)),
        out_specs=VMEM_SPEC,
        out_shape=pltpu.HBM((n, d), jnp.bfloat16),
        scratch_shapes=[pltpu.VMEM((m, d), jnp.bfloat16)],
        compiler_params=pltpu.CompilerParams(vmem_limit_bytes=16 * MIB),
        cost_estimate=pl.CostEstimate(
            flops=2 * n * m * d, bytes_accessed=2 * d * (n + m), transcendentals=0
        ),
    )(*in_hbm(chosen, *blocks))


def weigh_kernel(high, low, rows, *outs):
    cut(weighted_sum(high[...], low[...], rows[...]), outs)


def weigh_late(high, low, rows):
    n, d = rows.shape
    sizes = [LANES] * len(OFFSETS)
    return pl.pallas_call(
        weigh_kernel,
        in_specs=[VMEM_SPEC] * 3,
        out_specs=[VMEM_SPEC] * len(sizes),
        out_shape=[pltpu.HBM((s, d), jnp.bfloat16) for s in sizes],
        compiler_params=pltpu.CompilerParams(vmem_limit_bytes=16 * MIB),
        cost_estimate=pl.CostEstimate(
            flops=4 * n * LANES * len(OFFSETS) * d, bytes_accessed=6 * d * n, transcendentals=0
        ),
    )(high, low, rows)


def finish_kernel(high, low, rows, own, left, right, far, out):
    value = weighted_sum(high[...], low[...], rows[...])
    for part in (own, left, right, far):
        value = value + part[...].astype(jnp.float32)
    out[...] = value.astype(out.dtype)


def finish(high, low, rows, parts):
    n, d = rows.shape
    return pl.pallas_call(
        finish_kernel,
        in_specs=[VMEM_SPEC] * (3 + len(parts)),
        out_specs=VMEM_SPEC,
        out_shape=jax.ShapeDtypeStruct((LANES, d), jnp.bfloat16),
        compiler_params=pltpu.CompilerParams(vmem_limit_bytes=16 * MIB),
        cost_estimate=pl.CostEstimate(
            flops=4 * n * LANES * d, bytes_accessed=2 * d * (n + 4 * LANES), transcendentals=0
        ),
    )(high, low, rows, *parts)


def send_near(to_left, to_right):
    got_bottom = shift(to_left, -1)
    got_top = shift(to_right, 1)
    return got_top, got_bottom


def send_far(far_top, far_bottom):
    return shift(far_top, -1), shift(far_bottom, 1)


def send_on(to_left, to_right, via_right, via_left):
    left, right = add_pairs(to_left, via_right, to_right, via_left)
    return shift(left, -1), shift(right, 1)


def per_device(tokens, norm_gain, expert_ids, route_weight, exp_gate, exp_up, exp_down):
    experts_all = lax.axis_size(EP)
    me = lax.axis_index("tp").reshape(1)
    ids, route = expert_ids.T, route_weight.T

    normed, sent = prepare(tokens, norm_gain, ids, me, experts_all)
    blocks = gather_tp(normed)
    arrived = exchange(sent)
    arrived, blocks = lax.optimization_barrier((arrived, blocks))

    late_chosen, late_high, late_low, high, low = route_tables(me, ids, route, experts_all)
    late_sent = select_late(late_chosen, blocks)
    late_arrived = exchange(late_sent)

    mid = arrived.shape[0] // 2
    top, bottom = arrived[:mid], arrived[mid:]
    left_top, right_bottom = shift(top, 1), shift(bottom, -1)
    left_bottom, right_top = shift(bottom, 1), shift(top, -1)
    far_top, far_bottom = shift(left_top, 1), shift(right_bottom, -1)
    weights = (exp_gate, exp_up, exp_down)
    *first, gate_tiles, up_tiles, down_tiles = expert_streamed(
        [left_top, right_bottom], [mid] * 2, weights, True
    )
    tiles = (gate_tiles, up_tiles, down_tiles)
    left_bottom, right_top, first = lax.optimization_barrier((left_bottom, right_top, first))
    second = expert_kept([left_bottom, right_top], [mid] * 2, tiles)
    near = send_near(*second)
    far_top, far_bottom, second = lax.optimization_barrier((far_top, far_bottom, second))
    third = expert_kept([far_top, far_bottom], [mid] * 2, tiles)
    via = send_far(*third)
    late_arrived, _ = lax.optimization_barrier((late_arrived, third))
    (late_part,) = expert_streamed([late_arrived], [late_arrived.shape[0]], weights, False)
    late_back = exchange(late_part)
    on = send_on(*first, *via)
    own_rows, _ = lax.optimization_barrier((arrived, (late_part, via)))
    (own_part,) = expert_streamed([own_rows], [2 * mid], weights, False)
    summed = jnp.concatenate(near, axis=0).astype(jnp.float32)
    summed = summed + jnp.concatenate(on, axis=0).astype(jnp.float32)
    summed = (summed + own_part.astype(jnp.float32)).astype(jnp.bfloat16)
    back = exchange(summed)

    late_back, _ = lax.optimization_barrier((late_back, own_part))
    sums = weigh_late(late_high, late_low, late_back)
    token_own, left, right, far = sums
    token_far = shift(far, 2)
    token_left, token_right = shift(left, -1), shift(right, 1)
    return finish(high, low, back, (token_own, token_left, token_right, token_far))


def solution(mesh):
    finer = Mesh(mesh.devices.reshape(4, 4, 2, mesh.shape["tp"]), ("ep_0", "ep_1", "ep_2", "tp"))
    return jax.shard_map(
        per_device,
        mesh=finer,
        in_specs=(
            P(EP_TP, None),
            P(),
            P(EP, None),
            P(EP, None),
            P(EP, None, "tp"),
            P(EP, None, "tp"),
            P(EP, "tp", None),
        ),
        out_specs=P(EP_TP, None),
        check_vma=False,
    )
```
